32 devices in a mesh: ep: 8 (over z, core), tp: 4 (over y, x).
Axes of the slice: x: 2, y: 2, z: 4, core: 2. Of those that a mesh axis runs over, the one named last changes fastest.
Arguments:
- query_rows: bfloat16 [3072, 2048], P('ep', 'tp'), may hold values from -6 to 6
- key_rows: bfloat16 [3072, 2048], P('ep', 'tp'), may hold values from -6 to 6
- value_rows: bfloat16 [3072, 2048], P('ep', 'tp'), may hold values from -6 to 6
- second_scale: float32 [16], P('tp'), may hold values from 0.3 to 0.8
- head_gain: float32 [128], replicated, may hold values from 0.1 to 1.9
- out_weight: bfloat16 [2048, 4096], P(None, 'tp'), may hold values from -0.125 to 0.125
- routed_rows: bfloat16 [1024, 4096], P('ep', 'tp'), may hold values from -6 to 6
- norm_gain: float32 [4096], replicated, may hold values from 0.1 to 1.9
- route_ids: int32 [1024, 2], P('ep'), may hold values from 0 to 7, all different within a row; in each aligned block of 128 rows (0 to 127, 128 to 255, ...) at most 64 rows name the same one
- route_weight: float32 [1024, 2], P('ep'), may hold values from 0.1 to 0.9
- expert_gate: bfloat16 [8, 4096, 2048], P('ep', None, 'tp'), may hold values from -0.09375 to 0.09375
- expert_up: bfloat16 [8, 4096, 2048], P('ep', None, 'tp'), may hold values from -0.09375 to 0.09375
- expert_down: bfloat16 [8, 2048, 4096], P('ep', None, 'tp'), may hold values from -0.125 to 0.125
Outputs:
- mixer_out: bfloat16 [3072, 4096], P('ep', 'tp')
- expert_mix: bfloat16 [1024, 4096], P('ep', 'tp')
The draws below stay inside these ranges and needn't reach their ends.
Inputs may be any that keep to these rules, and one draw needn't show every extreme that they name: `route_ids`: among the 128 tokens of one index of ep, no expert is named by more than 64 of them, a bound that some block reaches.
All inputs are finite; a program needn't handle non-finite values.
Results may differ from the reference program's by a relative error of at most 0.0085.
Values may be sent and summed in bfloat16 or wider, within the bound.
No kernel may reach another device: no remote copies, remote signals or barrier semaphores. Data moves between devices by JAX's collectives and lax.ppermute only.
A program may use at most 128 MiB of HBM per device.

```python
import math
import jax
import jax.numpy as jnp
import numpy as np
from jax import lax

D = 4096
HEADS = 16
HD = 64
VD = 128
FF = 2048
TOP = 2
TOK_A = 384
TOK_B = 128
TOKENS_A = 3072
TOKENS_B = 1024
EXPERTS = 8
CAP = 64
N_EP = 8


def draw_query_rows(key, part):
    length_all = TOK_A * N_EP
    drawn_rows = jnp.clip(1.3 * jax.random.normal(jax.random.fold_in(key, 3), (length_all, HEADS * 2 * HD), jnp.float32), -6.0, 6.0)
    return drawn_rows.astype(jnp.bfloat16)


def draw_key_rows(key, part):
    length_all = TOK_A * N_EP
    drawn_rows = jnp.clip(1.3 * jax.random.normal(jax.random.fold_in(key, 5), (length_all, HEADS * 2 * HD), jnp.float32), -6.0, 6.0)
    return drawn_rows.astype(jnp.bfloat16)


def level_of(rng, shape, split, smallest, largest):
    factor_of = 1.0
    for axis_at, parts in split:
        draws = jax.random.uniform(jax.random.fold_in(jax.random.fold_in(rng, 6), axis_at), (parts,), jnp.float32, smallest / len(split), largest / len(split))
        factor_of = factor_of * jnp.repeat(jnp.exp(draws), shape[axis_at] // parts).reshape((-1,) + (1,) * (len(shape) - 1 - axis_at))
    return factor_of


def deal_out(stream_key, own, number, rows, number_of, top, bound, slope):
    order = jax.random.permutation(stream_key, number_of)
    crowded, ordinary = load_shares(number_of, rows * top, bound, slope, True), load_shares(number_of, rows * top, bound, slope, False)
    places = jnp.arange(number_of)

    def named(sizes, offset_by):
        used = int((sizes > 0).sum())
        fixed = max(1, used // 4)
        passed = fixed + (places - fixed + offset_by * (used - fixed)) % max(1, number_of - fixed)
        return jnp.zeros((number_of,), jnp.int32).at[order[jnp.where(places < fixed, places, passed)]].set(jnp.asarray(sizes, jnp.int32))

    sizes = jnp.where(number % 4 == 0, named(crowded, number // 4), named(ordinary, number - number // 4 - 1))
    mixed = jax.random.permutation(jax.random.fold_in(own, 3), number_of)
    giver, sink = mixed[0:number_of // 2 * 2:2], mixed[1:number_of // 2 * 2:2]
    margin = jnp.minimum(sizes[giver] - 1, bound - sizes[sink]) // 2
    margin = jnp.where((giver == order[0]) | (sink == order[0]) | (sizes[sink] == 0), 0, jnp.maximum(margin, 0))
    passed = jax.random.randint(jax.random.fold_in(own, 4), (number_of // 2,), 0, 1 << 20) % (margin + 1)
    sizes = sizes.at[giver].add(-passed).at[sink].add(passed)
    labels = jnp.searchsorted(jnp.cumsum(sizes), jnp.arange(rows * top), side="right").astype(jnp.int32)
    table = labels.reshape(top, rows).T
    table = table[jax.random.permutation(jax.random.fold_in(own, 1), rows)]
    offset_by = jax.random.randint(jax.random.fold_in(own, 2), (rows, 1), 0, top)
    return jnp.take_along_axis(table, (jnp.arange(top)[None, :] + offset_by) % top, axis=1)


def load_shares(amount, total, limit, slope, full):
    loads = [(1 << 20) // math.isqrt(rank ** slope) + 1 for rank in range(1, amount + 1)]
    largest = limit if full else min(limit, max(-(-total // amount), total * loads[0] // sum(loads)))
    least = 1 if total - largest >= amount - 1 else 0
    given, spare = [largest] + [least] * (amount - 1), total - largest - least * (amount - 1)
    while spare > 0:
        free = [i for i in range(1, amount) if given[i] < largest] or [i for i in range(1, amount) if given[i] < limit]
        pool, remaining = sum([loads[i] for i in free]), spare
        for i in free:
            more = min(limit - given[i], max(1, remaining * loads[i] // pool), spare)
            given[i] = given[i] + more
            spare = spare - more
    return np.array(given)


def normal_values(key, dims, spread, reach, pieces=(), held_as=jnp.bfloat16):
    level = level_of(key, dims, pieces, -0.22, 0.18) if pieces else 1.0
    values = jax.random.normal(key, dims, jnp.float32) * spread * level
    return jnp.minimum(jnp.maximum(values, -reach), reach).astype(held_as)


def setup_inputs(seed: int = 0) -> dict:
    keys = jax.random.split(jax.random.key(seed), 14)
    query_rows = draw_query_rows(jax.random.fold_in(keys[13], 71), 0)
    key_rows = draw_key_rows(jax.random.fold_in(keys[13], 71), 0)
    value_rows = normal_values(keys[2], (TOKENS_A, HEADS * VD), 1.0, 6.0, ((0, 8), (1, 4)))
    second_scale = jnp.clip(0.3 + 0.5 * jax.random.uniform(keys[3], (HEADS,), jnp.float32) ** level_of(keys[3], (HEADS,), ((0, 4),), -0.2, 0.2), 0.3, 0.8)
    head_gain = jnp.clip(1.0 + 0.18 * jax.random.normal(keys[4], (VD,), jnp.float32), 0.1, 1.9)
    out_weight = normal_values(keys[5], (HEADS * VD, D), (HEADS * VD) ** -0.5, 0.125, ((1, 4),))
    routed_rows = normal_values(keys[6], (TOKENS_B, D), 1.0, 6.0, ((0, 8), (1, 4)))
    norm_gain = jnp.clip(1.0 + 0.18 * jax.random.normal(keys[7], (D,), jnp.float32), 0.1, 1.9)
    route_ids_keys = jax.random.split(jax.random.fold_in(keys[8], 1), TOKENS_B // TOK_B)
    route_ids_turns = jax.random.permutation(jax.random.fold_in(keys[8], 3), TOKENS_B // TOK_B)
    route_ids = jax.vmap(lambda own, number: deal_out(jax.random.fold_in(keys[8], 2), own, number, TOK_B, EXPERTS, TOP, CAP, 1))(route_ids_keys, route_ids_turns).reshape((TOKENS_B, TOP))
    route_weight = jnp.clip(0.1 + 0.79999997 * jax.random.uniform(keys[9], (TOKENS_B, TOP), jnp.float32) ** level_of(keys[9], (TOKENS_B, TOP), ((0, 8),), -0.2, 0.2), 0.1, 0.9)
    expert_gate = normal_values(keys[10], (EXPERTS, D, FF), D ** -0.5, 0.09375, ((0, 8), (2, 4)))
    expert_up = normal_values(keys[11], (EXPERTS, D, FF), D ** -0.5, 0.09375, ((0, 8), (2, 4)))
    expert_down = normal_values(keys[12], (EXPERTS, FF, D), FF ** -0.5, 0.125, ((0, 8), (2, 4)))
    return {"query_rows": query_rows, "key_rows": key_rows, "value_rows": value_rows, "second_scale": second_scale, "head_gain": head_gain, "out_weight": out_weight, "routed_rows": routed_rows, "norm_gain": norm_gain, "route_ids": route_ids, "route_weight": route_weight, "expert_gate": expert_gate, "expert_up": expert_up, "expert_down": expert_down}


eps = 1e-06
head_factor = 0.8
neg_big = -1e+30

def rms_rows(rows_in, gain):
    floats = rows_in.astype(jnp.float32)
    factor = lax.rsqrt(lax.optimization_barrier(jnp.mean(floats * floats, axis=-1, keepdims=True)) + eps)
    return (floats * factor * gain).astype(jnp.bfloat16)

def reference(query_rows, key_rows, value_rows, second_scale, head_gain, out_weight, routed_rows, norm_gain, route_ids, route_weight, expert_gate, expert_up, expert_down):
    length_all = query_rows.shape[0]
    block_rows = min(512, length_all)
    positions = jnp.arange(length_all, dtype=jnp.int32)
    query_heads = jnp.transpose(query_rows.reshape(length_all, HEADS, 2, HD), (1, 0, 2, 3))
    key_heads = jnp.transpose(key_rows.reshape(length_all, HEADS, 2, HD), (1, 0, 2, 3))
    value_heads = jnp.transpose(value_rows.reshape(length_all, HEADS, VD), (1, 0, 2))

    def one_head(operands):
        query_h, key_h, value_h, scale_h = operands
        key_float = key_h.astype(jnp.float32)
        value_float = value_h.astype(jnp.float32)

        def one_block(block_num):
            row_first = block_num * block_rows
            query_block = lax.dynamic_slice_in_dim(query_h, row_first, block_rows, 0).astype(jnp.float32)
            scores = jnp.einsum('icd,jcd->cij', query_block, key_float) * HD ** (-0.5)
            allowed = ((row_first + jnp.arange(block_rows, dtype=jnp.int32))[:, None] >= positions[None, :])[None]
            scores = jnp.where(allowed, scores, neg_big)
            row_max = lax.optimization_barrier(jnp.max(scores, axis=-1, keepdims=True))
            exp_scores = jnp.where(allowed, jnp.exp(scores - row_max), 0.0)
            denoms = lax.optimization_barrier(jnp.sum(exp_scores, axis=-1))
            rounded = lax.optimization_barrier(exp_scores.astype(jnp.bfloat16)).astype(jnp.float32)
            maps_both = jnp.einsum('cij,je->cie', rounded, value_float) / denoms[..., None]
            mixed_maps = maps_both[0] - scale_h * maps_both[1]
            mean_sq = lax.optimization_barrier(jnp.mean(mixed_maps * mixed_maps, axis=-1, keepdims=True))
            return (mixed_maps * lax.rsqrt(mean_sq + eps) * head_gain * head_factor).astype(jnp.bfloat16)
        block_outs = lax.map(one_block, jnp.arange(length_all // block_rows, dtype=jnp.int32))
        return block_outs.reshape(length_all, VD)
    head_outs = lax.map(one_head, (query_heads, key_heads, value_heads, second_scale))
    head_cat = jnp.transpose(head_outs, (1, 0, 2)).reshape(length_all, HEADS * VD)
    mixer_out = jnp.dot(head_cat, out_weight, preferred_element_type=jnp.float32).astype(jnp.bfloat16)
    normed = rms_rows(routed_rows, norm_gain)
    flat_expert = route_ids.reshape(-1).astype(jnp.int32)
    count_all = flat_expert.shape[0]
    chosen = (flat_expert[:, None] == jnp.arange(EXPERTS, dtype=jnp.int32)[None, :]).astype(jnp.int32)
    ranks = lax.optimization_barrier(jnp.sum((jnp.cumsum(chosen, axis=0) - 1) * chosen, axis=1)).astype(jnp.int32)
    token_of = jnp.arange(count_all, dtype=jnp.int32) // TOP
    table = jnp.full((EXPERTS, N_EP * CAP), TOKENS_B, jnp.int32).at[flat_expert, ranks].set(token_of)
    padded = jnp.concatenate([normed, jnp.zeros((1, D), jnp.bfloat16)], axis=0)

    def one_expert(operands):
        table_row, gate_w, up_w, down_w = operands
        gathered = padded[table_row]
        gate_val = jnp.dot(gathered, gate_w, preferred_element_type=jnp.float32)
        up_val = jnp.dot(gathered, up_w, preferred_element_type=jnp.float32)
        hidden = (jax.nn.silu(gate_val) * up_val).astype(jnp.bfloat16)
        return jnp.dot(hidden, down_w, preferred_element_type=jnp.float32).astype(jnp.bfloat16)
    expert_outs = lax.map(one_expert, (table, expert_gate, expert_up, expert_down))
    picked = expert_outs[flat_expert, ranks].astype(jnp.float32).reshape(TOKENS_B, TOP, D)
    expert_mix = lax.optimization_barrier(jnp.sum(picked * route_weight[:, :, None], axis=1)).astype(jnp.bfloat16)
    return (mixer_out, expert_mix)
```

```python
import functools

import jax
import jax.numpy as jnp
from jax import lax
from jax.experimental import pallas as pl
from jax.experimental.pallas import tpu as pltpu
from jax.sharding import PartitionSpec as P

eps = 1e-06
head_factor = 0.8
neg_big = -1e30
key_block_rows = 1024


def rms_rows(rows_in, gain):
    floats = rows_in.astype(jnp.float32)
    factor = lax.rsqrt(jnp.mean(floats * floats, axis=-1, keepdims=True) + eps)
    return (floats * factor * gain).astype(jnp.bfloat16)


def per_device(
    query_rows,
    key_rows,
    value_rows,
    second_scale,
    head_gain,
    out_weight,
    routed_rows,
    norm_gain,
    route_ids,
    route_weight,
    expert_gate,
    expert_up,
    expert_down,
):
    count_a = query_rows.shape[0]
    per_head = second_scale.shape[0]
    head_dim = query_rows.shape[1] // (2 * per_head)
    value_dim = head_gain.shape[0]
    query_four = query_rows.reshape(count_a, per_head, 2, head_dim)
    query_pos = lax.axis_index("ep") * count_a + jnp.arange(count_a, dtype=jnp.int32)

    def key_block(carry_state, key_part, value_part, block_start):
        key_count = key_part.shape[0]
        key_four = key_part.reshape(key_count, per_head, 2, head_dim)
        value_three = value_part.reshape(key_count, per_head, value_dim)
        scores = jnp.einsum(
            "ihcd,jhcd->ihcj", query_four, key_four, preferred_element_type=jnp.float32
        ) * head_dim ** (-0.5)
        allowed = (
            query_pos[:, None] >= block_start + jnp.arange(key_count, dtype=jnp.int32)[None, :]
        )[:, None, None, :]
        scores = jnp.where(allowed, scores, neg_big)
        old_max, old_sum, old_acc = carry_state
        new_max = jnp.maximum(old_max, jnp.max(scores, axis=-1))
        weights = jnp.where(allowed, jnp.exp(scores - new_max[..., None]), 0.0)
        shrink = jnp.exp(old_max - new_max)
        new_sum = old_sum * shrink + jnp.sum(weights, axis=-1)
        update = jnp.einsum(
            "ihcj,jhe->ihce",
            weights.astype(jnp.bfloat16),
            value_three,
            preferred_element_type=jnp.float32,
        )
        return (new_max, new_sum, old_acc * shrink[..., None] + update)

    start_state = (
        jnp.full((count_a, per_head, 2), neg_big, jnp.float32),
        jnp.zeros((count_a, per_head, 2), jnp.float32),
        jnp.zeros((count_a, per_head, 2, value_dim), jnp.float32),
    )
    key_part = lax.all_gather(key_rows, "ep", axis=0, tiled=True)
    value_part = lax.all_gather(value_rows, "ep", axis=0, tiled=True)
    key_count = key_part.shape[0]

    def step_block(block_num, inner_state):
        offset_rows = block_num * key_block_rows
        key_slice = lax.dynamic_slice_in_dim(key_part, offset_rows, key_block_rows, 0)
        value_slice = lax.dynamic_slice_in_dim(value_part, offset_rows, key_block_rows, 0)
        return key_block(inner_state, key_slice, value_slice, offset_rows)

    run_max, run_sum, run_acc = lax.fori_loop(
        0, key_count // key_block_rows, step_block, start_state
    )
    maps_both = run_acc / run_sum[..., None]
    mixed_maps = maps_both[:, :, 0] - second_scale[None, :, None] * maps_both[:, :, 1]
    mean_sq = jnp.mean(mixed_maps * mixed_maps, axis=-1, keepdims=True)
    head_out = (
        (mixed_maps * lax.rsqrt(mean_sq + eps) * head_gain * head_factor)
        .astype(jnp.bfloat16)
        .reshape(count_a, per_head * value_dim)
    )
    count_b = routed_rows.shape[0]
    route_count = route_ids.shape[1]
    experts_here = expert_gate.shape[0]
    ep_devices = lax.axis_size("ep")
    expert_total = experts_here * ep_devices
    capacity = 2 * count_b * route_count // expert_total
    flat_expert = route_ids.reshape(-1)
    chosen = (flat_expert[:, None] == jnp.arange(expert_total, dtype=jnp.int32)[None, :]).astype(
        jnp.int32
    )
    ranks = jnp.sum((jnp.cumsum(chosen, axis=0) - 1) * chosen, axis=1)
    slot_of = flat_expert * capacity + ranks
    token_of = jnp.arange(count_b * route_count, dtype=jnp.int32) // route_count
    slot_token = jnp.full((expert_total * capacity,), count_b, jnp.int32).at[slot_of].set(token_of)
    padded = jnp.concatenate(
        [routed_rows, jnp.zeros((1, routed_rows.shape[1]), jnp.bfloat16)], axis=0
    )
    outgoing = padded[slot_token].reshape(ep_devices, experts_here, capacity, routed_rows.shape[1])
    column_parts = lax.all_to_all(outgoing, "ep", split_axis=0, concat_axis=0, tiled=True)
    arrived = rms_rows(lax.all_gather(column_parts, "tp", axis=3, tiled=True), norm_gain)
    gate_val = jnp.einsum(
        "sxcd,xdf->sxcf", arrived, expert_gate, preferred_element_type=jnp.float32
    )
    up_val = jnp.einsum("sxcd,xdf->sxcf", arrived, expert_up, preferred_element_type=jnp.float32)
    hidden = (jax.nn.silu(gate_val) * up_val).astype(jnp.bfloat16)
    weight_rows = out_weight
    attn_total = jnp.dot(
        lax.all_gather(
            head_out.reshape(1, 1, count_a, head_out.shape[1]), "tp", axis=3, tiled=True
        )[0, 0],
        weight_rows,
        preferred_element_type=jnp.float32,
    )
    weight_rows = expert_down
    moe_total = jnp.einsum(
        "sxcf,xfd->sxcd",
        lax.all_gather(hidden, "tp", axis=3, tiled=True),
        weight_rows,
        preferred_element_type=jnp.float32,
    )
    mixer_out = attn_total.astype(jnp.bfloat16)
    returned = lax.all_to_all(
        moe_total.astype(jnp.bfloat16), "ep", split_axis=0, concat_axis=0, tiled=True
    )
    flat_back = returned.reshape(expert_total * capacity, returned.shape[3])
    picked = flat_back[slot_of].astype(jnp.float32).reshape(count_b, route_count, returned.shape[3])
    expert_mix = jnp.sum(picked * route_weight[:, :, None], axis=1).astype(jnp.bfloat16)
    return (mixer_out, expert_mix)


bf16 = jnp.bfloat16
f32 = jnp.float32
vmem = pl.BlockSpec(memory_space=pltpu.VMEM)
smem = pl.BlockSpec(memory_space=pltpu.SMEM)
vmem_bytes = 56 * 1024 * 1024


def params(**more):
    return pltpu.CompilerParams(vmem_limit_bytes=vmem_bytes, **more)


def sds(*shape):
    return jax.ShapeDtypeStruct(shape, bf16)


def pack_kernel(width, where_ref, q_ref, k_ref, v_ref, *outs):
    chip = where_ref[0]
    scale = (width // 2) ** (-0.5)
    for slot, out in enumerate(outs):
        at = pl.ds(pl.multiple_of((chip ^ slot) * width, width), width)
        out[:, 0:width] = (q_ref[:, at].astype(f32) * scale).astype(bf16)
        out[:, width : 2 * width] = k_ref[:, at]
        out[:, 2 * width : 3 * width] = v_ref[:, at]


def attention_kernel(chips, count, width, where_ref, scale_ref, gain_ref, *refs):
    own, other = refs[:chips], refs[chips : 2 * chips]
    outs = refs[2 * chips : 3 * chips]
    keys, values, queries, scores, acc, row_max, row_sum = refs[3 * chips :]
    chip, core = where_ref[0], where_ref[1]
    half = width // 2
    pair = 2 * count
    for slot in range(chips):
        at = chip ^ slot
        for parity, part in ((core, own[slot]), (1 - core, other[slot])):
            rows = pl.ds(pl.multiple_of(parity * count, count), count)
            keys[at, rows] = part[:, width : 2 * width]
            values[at, rows] = part[:, 2 * width : 3 * width]
    lane = lax.broadcasted_iota(jnp.int32, (count, width), 1)

    def widest(block):
        best = block[:, 0:width]
        for i in range(width, pair, width):
            best = jnp.maximum(best, block[:, i : i + width])
        return best

    def products(number):
        return lax.dot_general(
            queries[...], keys[number], (((1,), (1,)), ((), ())), preferred_element_type=f32
        )

    def weigh(number):
        top = row_max[...]
        block = [
            jnp.exp(scores[number, :, i : i + width] - top) for i in range(0, pair, width)
        ]
        total = functools.reduce(jnp.add, block)
        weights = jnp.concatenate([part.astype(bf16) for part in block], axis=1)
        return total, jnp.dot(weights, values[number], preferred_element_type=f32)

    for slot in range(chips):
        last = chip ^ slot
        rows = own[slot][:, 0:width]
        queries[0:count] = jnp.where(lane < half, rows, jnp.zeros_like(rows))
        queries[count:pair] = jnp.where(lane < half, jnp.zeros_like(rows), rows)
        allowed = lax.broadcasted_iota(jnp.int32, (pair, pair), 1) <= (
            lax.broadcasted_iota(jnp.int32, (pair, pair), 0) % count + core * count
        )
        masked = jnp.where(allowed, products(last), neg_big)
        scores[last] = masked
        row_max[...] = widest(masked)

        @pl.loop(0, last)
        def _(number):
            block = products(number)
            scores[number] = block
            row_max[...] = jnp.maximum(row_max[...], widest(block))

        row_max[...] = jnp.broadcast_to(
            jnp.max(row_max[...], axis=-1, keepdims=True), row_max.shape
        )
        row_sum[...], acc[...] = weigh(last)

        @pl.loop(0, last)
        def _(number):
            total, update = weigh(number)
            row_sum[...] += total
            acc[...] += update

        maps = acc[...] / jnp.sum(row_sum[...], axis=-1, keepdims=True)
        mixed = maps[0:count] - scale_ref[chip] * maps[count:pair]
        mean_sq = jnp.mean(mixed * mixed, axis=-1, keepdims=True)
        outs[slot][...] = (
            mixed * lax.rsqrt(mean_sq + eps) * gain_ref[...] * head_factor
        ).astype(bf16)


def project_kernel(parts, groups, width, where_ref, w_ref, *refs):
    pieces, (out, heads, acc) = refs[: len(groups) * parts], refs[-3:]
    step = pl.program_id(0)
    chip = where_ref[0]
    for part in range(parts):

        @pl.when(step == part)
        def _():
            for number, slots in enumerate(groups):
                for i, slot in enumerate(slots):
                    at = pl.ds(pl.multiple_of((chip ^ slot) * width, width), width)
                    heads[:, at] = pieces[number * parts + part][:, i * width : (i + 1) * width]

    product = jnp.dot(heads[...], w_ref[...], preferred_element_type=f32)

    @pl.when(step == 0)
    def _():
        acc[...] = product

    @pl.when((step > 0) & (step < parts - 1))
    def _():
        acc[...] += product

    @pl.when(step == parts - 1)
    def _():
        out[...] = (acc[...] + product).astype(bf16)


def select_kernel(count, routes, capacity, groups, where_ref, *refs):
    slots = [slot for group in groups for slot in group]
    own, other, outs = refs[: len(slots)], refs[len(slots) : 2 * len(slots)], refs[2 * len(slots) :]
    expert = (2 * where_ref[0] + where_ref[1]).astype(f32)
    before = (
        lax.broadcasted_iota(jnp.int32, (count, count), 0)
        < lax.broadcasted_iota(jnp.int32, (count, count), 1)
    ).astype(f32).astype(bf16)
    row_of = lax.broadcasted_iota(jnp.int32, (capacity, count), 0).astype(f32)
    at = 0
    for out, group in zip(outs, groups):
        for i in range(len(group)):
            for side, part in ((0, own[at]), (1, other[at])):
                ids = part[count : count + 8, 0:count].astype(f32)
                chosen = jnp.zeros((1, count), f32)
                for k in range(routes):
                    chosen = jnp.where(ids[k : k + 1] == expert, 1.0, chosen)
                rank = jnp.dot(
                    jnp.broadcast_to(chosen, (8, count)).astype(bf16),
                    before,
                    preferred_element_type=f32,
                )[0:1]
                rank = jnp.where(chosen > 0, rank, -1.0)
                pick = jnp.where(row_of == rank, 1.0, 0.0).astype(bf16)
                first = (2 * i + side) * capacity
                out[first : first + capacity] = jnp.dot(
                    pick, part[0:count], preferred_element_type=f32
                ).astype(bf16)
            at += 1


def gate_up_kernel(parts, rows_per, width, where_ref, gain_ref, gate_ref, up_ref, *refs):
    groups = len(rows_per)
    pieces, outs = refs[: groups * parts], refs[groups * parts : groups * (parts + 1)]
    rows, gate_acc, up_acc, squares = refs[groups * (parts + 1) :]
    step = pl.program_id(0)
    for part in range(parts):

        @pl.when(step == part)
        def _():
            start = 0
            for group in range(groups):
                at = pl.ds(start, rows_per[group])
                floats = pieces[group * parts + part][...].astype(f32)
                square = jnp.sum(floats * floats, axis=-1, keepdims=True)
                if part:
                    square = square + squares[at]
                squares[at] = square
                rows[at] = (floats * gain_ref[0]).astype(bf16)
                start += rows_per[group]

    gate = jnp.dot(rows[...], gate_ref[0], preferred_element_type=f32)
    up = jnp.dot(rows[...], up_ref[0], preferred_element_type=f32)

    @pl.when(step == 0)
    def _():
        gate_acc[...] = gate
        up_acc[...] = up

    @pl.when((step > 0) & (step < parts - 1))
    def _():
        gate_acc[...] += gate
        up_acc[...] += up

    @pl.when(step == parts - 1)
    def _():
        factor = lax.rsqrt(squares[...] * (1.0 / width) + eps)
        g = (gate_acc[...] + gate) * factor
        u = (up_acc[...] + up) * factor
        hidden = (g / (1.0 + jnp.exp(-g)) * u).astype(bf16)
        start = 0
        for group in range(groups):
            outs[group][...] = hidden[start : start + rows_per[group]]
            start += rows_per[group]


def down_kernel(parts, rows_per, capacity, where_ref, w_ref, *refs):
    groups = len(rows_per)
    pieces = refs[: groups * parts]
    outs, (rows, acc) = refs[groups * parts : -2], refs[-2:]
    step = pl.program_id(0)
    for part in range(parts):

        @pl.when(step == part)
        def _():
            start = 0
            for group in range(groups):
                rows[pl.ds(start, rows_per[group])] = pieces[group * parts + part][...]
                start += rows_per[group]

    product = jnp.dot(rows[...], w_ref[0], preferred_element_type=f32)

    @pl.when(step == 0)
    def _():
        acc[...] = product

    @pl.when((step > 0) & (step < parts - 1))
    def _():
        acc[...] += product

    @pl.when(step == parts - 1)
    def _():
        total = (acc[...] + product).astype(bf16)
        for i in range(total.shape[0] // capacity):
            at = i // 2 * capacity
            outs[i % 2][at : at + capacity] = total[i * capacity : (i + 1) * capacity]


def combine_kernel(chips, count, capacity, routes, where_ref, *refs):
    ids_refs, mine_ref, theirs_ref = refs[:chips], refs[chips], refs[chips + 1]
    outs, rows = refs[chips + 2 : 2 * chips + 2], refs[-1]
    chip, core = where_ref[0], where_ref[1]
    before = (
        lax.broadcasted_iota(jnp.int32, (count, count), 0)
        < lax.broadcasted_iota(jnp.int32, (count, count), 1)
    ).astype(f32).astype(bf16)
    row_of = lax.broadcasted_iota(jnp.int32, (capacity, count), 0).astype(f32)
    for slot, out in enumerate(outs):
        part = ids_refs[slot][count : count + 8, 0:count].astype(f32)
        terms = [[], [], []]
        for side, results in ((0, mine_ref), (1, theirs_ref)):
            rows[side * capacity : (side + 1) * capacity] = results[
                slot * capacity : (slot + 1) * capacity
            ]
            expert = (2 * chip + (core ^ side)).astype(f32)
            chosen = jnp.zeros((1, count), f32)
            share = [jnp.zeros((1, count), f32)] * 3
            for k in range(routes):
                same = part[k : k + 1] == expert
                chosen = jnp.where(same, 1.0, chosen)
                for i in range(3):
                    at = routes * (1 + i) + k
                    share[i] = jnp.where(same, part[at : at + 1], share[i])
            rank = jnp.dot(
                jnp.broadcast_to(chosen, (8, count)).astype(bf16),
                before,
                preferred_element_type=f32,
            )[0:1]
            rank = jnp.where(chosen > 0, rank, -1.0)
            for i in range(3):
                terms[i].append(jnp.where(row_of == rank, share[i], 0.0).astype(bf16))
        total = jnp.zeros(out.shape, f32)
        for i in range(3):
            total = total + lax.dot_general(
                jnp.concatenate(terms[i], axis=0),
                rows[...],
                (((0,), (0,)), ((), ())),
                preferred_element_type=f32,
            )
        out[...] = total.astype(bf16)


def per_device_fast(
    query_rows,
    key_rows,
    value_rows,
    second_scale,
    head_gain,
    out_weight,
    routed_rows,
    norm_gain,
    route_ids,
    route_weight,
    expert_gate,
    expert_up,
    expert_down,
):
    ep_devices, tp_devices = lax.axis_size("ep"), lax.axis_size("tp")
    chips = ep_devices // 2
    count_a, count_b = query_rows.shape[0], routed_rows.shape[0]
    heads_here = second_scale.shape[0]
    width = query_rows.shape[1] // heads_here
    columns = routed_rows.shape[1]
    model = columns * tp_devices
    routes = route_ids.shape[1]
    capacity = 2 * count_b * routes // ep_devices
    units = expert_gate.shape[2]
    out_columns = out_weight.shape[1]
    ep_at = lax.axis_index("ep")
    where = jnp.stack([ep_at // 2, ep_at % 2, lax.axis_index("tp")]).astype(jnp.int32)

    def over_ep(value, slot, cross=0):
        pairs = [(i, (((i // 2) ^ slot) * 2 + (i % 2)) ^ cross) for i in range(ep_devices)]
        return lax.ppermute(value, "ep", pairs)

    def over_tp(value, offset):
        return lax.ppermute(value, "tp", [(i, i ^ offset) for i in range(tp_devices)])

    def spread(value, first, second):
        one = over_tp(value, first)
        pieces = {0: value, first: one, second: over_tp(value, second), 3: over_tp(one, second)}
        return [pieces[offset] for offset in range(tp_devices)]

    def call(body, out_shape, *args, scratch=(), scalars=0):
        return pl.pallas_call(
            body,
            out_shape=out_shape,
            in_specs=[smem] * (1 + scalars) + [vmem] * (len(args) - scalars),
            out_specs=jax.tree.map(lambda _: vmem, out_shape),
            scratch_shapes=list(scratch),
            compiler_params=params(),
        )(where, *args)

    table, rest = [route_ids.astype(f32)], route_weight
    for _ in range(3):
        table.append(rest.astype(bf16).astype(f32))
        rest = rest - table[-1]
    table = jnp.concatenate(table, axis=1).T.astype(bf16)
    ids_rows = jnp.pad(table, ((0, 0), (0, columns - count_b)))
    packed = jnp.concatenate([routed_rows, ids_rows], axis=0)
    arrived = [packed] + [over_ep(packed, slot) for slot in range(1, chips)]
    swapped = [over_ep(part, 0, 1) for part in arrived]

    packs = call(
        functools.partial(pack_kernel, width),
        [sds(count_a, 3 * width)] * chips,
        query_rows,
        key_rows,
        value_rows,
    )
    mine = [packs[0]] + [over_ep(packs[slot], slot) for slot in range(1, chips)]
    theirs = [over_ep(part, 0, 1) for part in mine]

    gain_parts = norm_gain.reshape(tp_devices, 1, columns)
    slots = [slot for group in row_groups for slot in group]
    rows_per = [2 * capacity * len(group) for group in row_groups]
    total = sum(rows_per)
    pieces = []
    for number, group in enumerate(row_groups):
        (picked,) = call(
            functools.partial(select_kernel, count_b, routes, capacity, [group]),
            [sds(rows_per[number], columns)],
            *[arrived[slot] for slot in group],
            *[swapped[slot] for slot in group],
        )
        pieces += spread(picked, *((1, 2) if number % 2 == 0 else (2, 1)))
    hidden = pl.pallas_call(
        functools.partial(gate_up_kernel, tp_devices, rows_per, model),
        out_shape=[sds(rows, units) for rows in rows_per],
        grid_spec=pltpu.PrefetchScalarGridSpec(
            num_scalar_prefetch=1,
            grid=(tp_devices,),
            in_specs=[
                pl.BlockSpec((1, 1, columns), lambda m, w: (w[2] ^ m, 0, 0)),
                pl.BlockSpec((1, columns, units), lambda m, w: (0, w[2] ^ m, 0)),
                pl.BlockSpec((1, columns, units), lambda m, w: (0, w[2] ^ m, 0)),
            ]
            + [vmem] * len(pieces),
            out_specs=[vmem] * len(rows_per),
            scratch_shapes=[
                pltpu.VMEM((total, columns), bf16),
                pltpu.VMEM((total, units), f32),
                pltpu.VMEM((total, units), f32),
                pltpu.VMEM((total, 1), f32),
            ],
        ),
        compiler_params=params(),
    )(where, gain_parts, expert_gate, expert_up, *pieces)
    pieces = []
    for number, value in enumerate(hidden):
        pieces += spread(value, *((1, 2) if number % 2 == 0 else (2, 1)))
    own_side, other_side = pl.pallas_call(
        functools.partial(down_kernel, tp_devices, rows_per, capacity),
        out_shape=[sds(capacity * len(slots), columns)] * 2,
        grid_spec=pltpu.PrefetchScalarGridSpec(
            num_scalar_prefetch=1,
            grid=(tp_devices,),
            in_specs=[pl.BlockSpec((1, units, columns), lambda m, w: (0, w[2] ^ m, 0))]
            + [vmem] * len(pieces),
            out_specs=[vmem] * 2,
            scratch_shapes=[
                pltpu.VMEM((total, units), bf16),
                pltpu.VMEM((total, columns), f32),
            ],
        ),
        compiler_params=params(),
    )(where, expert_down, *pieces)
    mixes = call(
        functools.partial(combine_kernel, chips, count_b, capacity, routes),
        [sds(count_b, columns)] * chips,
        *arrived,
        own_side,
        over_ep(other_side, 0, 1),
        scratch=[pltpu.VMEM((2 * capacity, columns), bf16)],
    )
    mixes = [mixes[0]] + [over_ep(mixes[slot], slot) for slot in range(1, chips)]
    expert_mix = functools.reduce(jnp.add, [part.astype(f32) for part in mixes]).astype(bf16)

    head_outs = call(
        functools.partial(attention_kernel, chips, count_a, width),
        [sds(count_a, width)] * chips,
        second_scale.reshape(heads_here),
        head_gain.reshape(1, width),
        *mine,
        *theirs,
        scalars=1,
        scratch=[
            pltpu.VMEM((chips, 2 * count_a, width), bf16),
            pltpu.VMEM((chips, 2 * count_a, width), bf16),
            pltpu.VMEM((2 * count_a, width), bf16),
            pltpu.VMEM((chips, 2 * count_a, 2 * count_a), f32),
            pltpu.VMEM((2 * count_a, width), f32),
            pltpu.VMEM((2 * count_a, width), f32),
            pltpu.VMEM((2 * count_a, width), f32),
        ],
    )
    back = [head_outs[0]] + [over_ep(head_outs[slot], slot) for slot in range(1, chips)]
    pieces = []
    for number, group in enumerate(head_groups):
        value = jnp.concatenate([back[slot] for slot in group], axis=1)
        pieces += spread(value, *((1, 2) if number % 2 == 0 else (2, 1)))
    depth = heads_here * width
    mixer_out = pl.pallas_call(
        functools.partial(project_kernel, tp_devices, head_groups, width),
        out_shape=sds(count_a, out_columns),
        grid_spec=pltpu.PrefetchScalarGridSpec(
            num_scalar_prefetch=1,
            grid=(tp_devices,),
            in_specs=[pl.BlockSpec((depth, out_columns), lambda m, w: (w[2] ^ m, 0))]
            + [vmem] * len(pieces),
            out_specs=vmem,
            scratch_shapes=[
                pltpu.VMEM((count_a, depth), bf16),
                pltpu.VMEM((count_a, out_columns), f32),
            ],
        ),
        compiler_params=params(),
    )(where, out_weight, *pieces)

    return (mixer_out, expert_mix)


row_groups = [(0, 1), (2, 3)]
head_groups = [(0, 1), (2, 3)]


def fast_fits(mesh):
    return mesh.shape["tp"] == 4 and mesh.shape["ep"] == 8


def solution(mesh):
    placed = (
        P("ep", "tp"),
        P("ep", "tp"),
        P("ep", "tp"),
        P("tp"),
        P(),
        P(None, "tp"),
        P("ep", "tp"),
        P(),
        P("ep", None),
        P("ep", None),
        P("ep", None, "tp"),
        P("ep", None, "tp"),
        P("ep", None, "tp"),
    )
    body = per_device_fast if fast_fits(mesh) else per_device
    return jax.shard_map(
        body,
        mesh=mesh,
        in_specs=placed,
        out_specs=(P("ep", "tp"), P("ep", "tp")),
        check_vma=False,
    )
```

```python
import functools

import jax
import jax.numpy as jnp
from jax import lax
from jax.experimental import pallas as pl
from jax.experimental.pallas import tpu as pltpu
from jax.sharding import PartitionSpec as P


eps = 1e-06
head_factor = 0.8
neg_big = -1e30
key_block_rows = 1024


def rms_rows(rows_in, gain):
    floats = rows_in.astype(jnp.float32)
    factor = lax.rsqrt(jnp.mean(floats * floats, axis=-1, keepdims=True) + eps)
    return (floats * factor * gain).astype(jnp.bfloat16)


def per_device(
    query_rows,
    key_rows,
    value_rows,
    second_scale,
    head_gain,
    out_weight,
    routed_rows,
    norm_gain,
    route_ids,
    route_weight,
    expert_gate,
    expert_up,
    expert_down,
):
    count_a = query_rows.shape[0]
    per_head = second_scale.shape[0]
    head_dim = query_rows.shape[1] // (2 * per_head)
    value_dim = head_gain.shape[0]
    query_four = query_rows.reshape(count_a, per_head, 2, head_dim)
    query_pos = lax.axis_index("ep") * count_a + jnp.arange(count_a, dtype=jnp.int32)

    def key_block(carry_state, key_part, value_part, block_start):
        key_count = key_part.shape[0]
        key_four = key_part.reshape(key_count, per_head, 2, head_dim)
        value_three = value_part.reshape(key_count, per_head, value_dim)
        scores = jnp.einsum(
            "ihcd,jhcd->ihcj", query_four, key_four, preferred_element_type=jnp.float32
        ) * head_dim ** (-0.5)
        allowed = (
            query_pos[:, None] >= block_start + jnp.arange(key_count, dtype=jnp.int32)[None, :]
        )[:, None, None, :]
        scores = jnp.where(allowed, scores, neg_big)
        old_max, old_sum, old_acc = carry_state
        new_max = jnp.maximum(old_max, jnp.max(scores, axis=-1))
        weights = jnp.where(allowed, jnp.exp(scores - new_max[..., None]), 0.0)
        shrink = jnp.exp(old_max - new_max)
        new_sum = old_sum * shrink + jnp.sum(weights, axis=-1)
        update = jnp.einsum(
            "ihcj,jhe->ihce",
            weights.astype(jnp.bfloat16),
            value_three,
            preferred_element_type=jnp.float32,
        )
        return (new_max, new_sum, old_acc * shrink[..., None] + update)

    start_state = (
        jnp.full((count_a, per_head, 2), neg_big, jnp.float32),
        jnp.zeros((count_a, per_head, 2), jnp.float32),
        jnp.zeros((count_a, per_head, 2, value_dim), jnp.float32),
    )
    key_part = lax.all_gather(key_rows, "ep", axis=0, tiled=True)
    value_part = lax.all_gather(value_rows, "ep", axis=0, tiled=True)
    key_count = key_part.shape[0]

    def step_block(block_num, inner_state):
        offset_rows = block_num * key_block_rows
        key_slice = lax.dynamic_slice_in_dim(key_part, offset_rows, key_block_rows, 0)
        value_slice = lax.dynamic_slice_in_dim(value_part, offset_rows, key_block_rows, 0)
        return key_block(inner_state, key_slice, value_slice, offset_rows)

    _, run_sum, run_acc = lax.fori_loop(0, key_count // key_block_rows, step_block, start_state)
    maps_both = run_acc / run_sum[..., None]
    mixed_maps = maps_both[:, :, 0] - second_scale[None, :, None] * maps_both[:, :, 1]
    mean_sq = jnp.mean(mixed_maps * mixed_maps, axis=-1, keepdims=True)
    head_out = (
        (mixed_maps * lax.rsqrt(mean_sq + eps) * head_gain * head_factor)
        .astype(jnp.bfloat16)
        .reshape(count_a, per_head * value_dim)
    )
    count_b = routed_rows.shape[0]
    route_count = route_ids.shape[1]
    experts_here = expert_gate.shape[0]
    ep_devices = lax.axis_size("ep")
    expert_total = experts_here * ep_devices
    capacity = 2 * count_b * route_count // expert_total
    flat_expert = route_ids.reshape(-1)
    chosen = (flat_expert[:, None] == jnp.arange(expert_total, dtype=jnp.int32)[None, :]).astype(
        jnp.int32
    )
    ranks = jnp.sum((jnp.cumsum(chosen, axis=0) - 1) * chosen, axis=1)
    slot_of = flat_expert * capacity + ranks
    token_of = jnp.arange(count_b * route_count, dtype=jnp.int32) // route_count
    slot_token = jnp.full((expert_total * capacity,), count_b, jnp.int32).at[slot_of].set(token_of)
    padded = jnp.concatenate(
        [routed_rows, jnp.zeros((1, routed_rows.shape[1]), jnp.bfloat16)], axis=0
    )
    outgoing = padded[slot_token].reshape(ep_devices, experts_here, capacity, routed_rows.shape[1])
    column_parts = lax.all_to_all(outgoing, "ep", split_axis=0, concat_axis=0, tiled=True)
    arrived = rms_rows(lax.all_gather(column_parts, "tp", axis=3, tiled=True), norm_gain)
    gate_val = jnp.einsum(
        "sxcd,xdf->sxcf", arrived, expert_gate, preferred_element_type=jnp.float32
    )
    up_val = jnp.einsum("sxcd,xdf->sxcf", arrived, expert_up, preferred_element_type=jnp.float32)
    hidden = (jax.nn.silu(gate_val) * up_val).astype(jnp.bfloat16)
    weight_rows = out_weight
    attn_total = jnp.dot(
        lax.all_gather(
            head_out.reshape(1, 1, count_a, head_out.shape[1]), "tp", axis=3, tiled=True
        )[0, 0],
        weight_rows,
        preferred_element_type=jnp.float32,
    )
    weight_rows = expert_down
    moe_total = jnp.einsum(
        "sxcf,xfd->sxcd",
        lax.all_gather(hidden, "tp", axis=3, tiled=True),
        weight_rows,
        preferred_element_type=jnp.float32,
    )
    mixer_out = attn_total.astype(jnp.bfloat16)
    returned = lax.all_to_all(
        moe_total.astype(jnp.bfloat16), "ep", split_axis=0, concat_axis=0, tiled=True
    )
    flat_back = returned.reshape(expert_total * capacity, returned.shape[3])
    picked = flat_back[slot_of].astype(jnp.float32).reshape(count_b, route_count, returned.shape[3])
    expert_mix = jnp.sum(picked * route_weight[:, :, None], axis=1).astype(jnp.bfloat16)
    return (mixer_out, expert_mix)


bf16 = jnp.bfloat16
f32 = jnp.float32
vmem = pl.BlockSpec(memory_space=pltpu.VMEM)
smem = pl.BlockSpec(memory_space=pltpu.SMEM)


def params(limit):
    return pltpu.CompilerParams(vmem_limit_bytes=limit * 1024 * 1024)


def near(value):
    return pltpu.with_memory_space_constraint(value, pltpu.VMEM)


def near_shapes(tree):
    return jax.tree.map(lambda leaf: pltpu.VMEM(leaf.shape, leaf.dtype), tree)


def sds(*shape):
    return jax.ShapeDtypeStruct(shape, bf16)


def pack_kernel(width, where_ref, q_ref, k_ref, v_ref, *outs):
    chip = where_ref[0]
    scale = (width // 2) ** (-0.5)
    for slot, out in enumerate(outs):
        at = pl.ds(pl.multiple_of((chip ^ slot) * width, width), width)
        out[:, 0:width] = (q_ref[:, at].astype(f32) * scale).astype(bf16)
        out[:, width : 2 * width] = k_ref[:, at]
        out[:, 2 * width : 3 * width] = v_ref[:, at]


def attention_kernel(chips, count, width, where_ref, scale_ref, gain_ref, *refs):
    own, other = refs[:chips], refs[chips : 2 * chips]
    outs = refs[2 * chips : 3 * chips]
    keys, values, queries, scores, acc, row_max, row_sum = refs[3 * chips :]
    chip, core = where_ref[0], where_ref[1]
    half = width // 2
    pair = 2 * count
    for slot in range(chips):
        at = chip ^ slot
        for parity, part in ((core, own[slot]), (1 - core, other[slot])):
            rows = pl.ds(pl.multiple_of(parity * count, count), count)
            keys[at, rows] = part[:, width : 2 * width]
            values[at, rows] = part[:, 2 * width : 3 * width]
    lane = lax.broadcasted_iota(jnp.int32, (count, width), 1)

    def widest(block):
        best = block[:, 0:width]
        for i in range(width, pair, width):
            best = jnp.maximum(best, block[:, i : i + width])
        return best

    def products(number):
        return lax.dot_general(
            queries[...], keys[number], (((1,), (1,)), ((), ())), preferred_element_type=f32
        )

    def weigh(number):
        top = row_max[...]
        block = [
            jnp.exp(scores[number, :, i : i + width] - top) for i in range(0, pair, width)
        ]
        total = functools.reduce(jnp.add, block)
        weights = jnp.concatenate([part.astype(bf16) for part in block], axis=1)
        return total, jnp.dot(weights, values[number], preferred_element_type=f32)

    for slot in range(chips):
        last = chip ^ slot
        rows = own[slot][:, 0:width]
        queries[0:count] = jnp.where(lane < half, rows, jnp.zeros_like(rows))
        queries[count:pair] = jnp.where(lane < half, jnp.zeros_like(rows), rows)
        allowed = lax.broadcasted_iota(jnp.int32, (pair, pair), 1) <= (
            lax.broadcasted_iota(jnp.int32, (pair, pair), 0) % count + core * count
        )
        masked = jnp.where(allowed, products(last), neg_big)
        scores[last] = masked
        row_max[...] = widest(masked)

        @pl.loop(0, last)
        def _(number):
            block = products(number)
            scores[number] = block
            row_max[...] = jnp.maximum(row_max[...], widest(block))

        row_max[...] = jnp.broadcast_to(
            jnp.max(row_max[...], axis=-1, keepdims=True), row_max.shape
        )
        row_sum[...], acc[...] = weigh(last)

        @pl.loop(0, last)
        def _(number):
            total, update = weigh(number)
            row_sum[...] += total
            acc[...] += update

        maps = acc[...] / jnp.sum(row_sum[...], axis=-1, keepdims=True)
        mixed = maps[0:count] - scale_ref[chip] * maps[count:pair]
        mean_sq = jnp.mean(mixed * mixed, axis=-1, keepdims=True)
        outs[slot][...] = (
            mixed * lax.rsqrt(mean_sq + eps) * gain_ref[...] * head_factor
        ).astype(bf16)


def project_kernel(parts, groups, width, where_ref, w_ref, *refs):
    pieces, (out, heads) = refs[: len(groups) * parts], refs[-2:]
    chip, tp = where_ref[0], where_ref[2]
    depth = heads.shape[1] // parts
    for part in range(parts):
        for number, slots in enumerate(groups):
            for i, slot in enumerate(slots):
                at = pl.multiple_of((tp ^ part) * depth + (chip ^ slot) * width, width)
                heads[:, pl.ds(at, width)] = pieces[number * parts + part][
                    :, i * width : (i + 1) * width
                ]
    out[...] = jnp.dot(heads[...], w_ref[...], preferred_element_type=f32).astype(bf16)


def rows_kernel(count, rows_ref, ids_ref, share_ref, out, ids, share, sems):
    copies = [
        pltpu.make_async_copy(rows_ref, out.at[0:count], sems.at[0]),
        pltpu.make_async_copy(ids_ref, ids, sems.at[1]),
        pltpu.make_async_copy(share_ref, share, sems.at[2]),
    ]
    for copy in copies:
        copy.start()
    out[count:] = jnp.zeros((out.shape[0] - count, out.shape[1]), bf16)
    copies[1].wait()
    copies[2].wait()
    table, rest = [ids[...].astype(f32)], share[...]
    for _ in range(3):
        table.append(rest.astype(bf16).astype(f32))
        rest = rest - table[-1]
    out[count:, 0:count] = jnp.concatenate(table, axis=0).astype(bf16)
    copies[0].wait()


def select_kernel(count, routes, capacity, groups, where_ref, *refs):
    slots = [slot for group in groups for slot in group]
    own, other, outs = refs[: len(slots)], refs[len(slots) : 2 * len(slots)], refs[2 * len(slots) :]
    expert = (2 * where_ref[0] + where_ref[1]).astype(f32)
    before = (
        lax.broadcasted_iota(jnp.int32, (count, count), 0)
        < lax.broadcasted_iota(jnp.int32, (count, count), 1)
    ).astype(f32).astype(bf16)
    row_of = lax.broadcasted_iota(jnp.int32, (capacity, count), 0).astype(f32)
    at = 0
    for out, group in zip(outs, groups):
        for i in range(len(group)):
            for side, part in ((0, own[at]), (1, other[at])):
                ids = part[count : count + 8, 0:count].astype(f32)
                chosen = jnp.zeros((1, count), f32)
                for k in range(routes):
                    chosen = jnp.where(ids[k : k + 1] == expert, 1.0, chosen)
                rank = jnp.dot(
                    jnp.broadcast_to(chosen, (8, count)).astype(bf16),
                    before,
                    preferred_element_type=f32,
                )[0:1]
                rank = jnp.where(chosen > 0, rank, -1.0)
                pick = jnp.where(row_of == rank, 1.0, 0.0).astype(bf16)
                first = (2 * i + side) * capacity
                out[first : first + capacity] = jnp.dot(
                    pick, part[0:count], preferred_element_type=f32
                ).astype(bf16)
            at += 1


def gate_up_kernel(parts, groups, where_ref, gain_ref, gate_ref, up_ref, *refs):
    pieces, (out, rows) = refs[: groups * parts], refs[-2:]
    tp = where_ref[2]
    width = rows.shape[1] // parts
    count = rows.shape[0] // groups
    factors = []
    for group in range(groups):
        square = jnp.zeros((count, 128), f32)
        for part in range(parts):
            floats = pieces[group * parts + part][...].astype(f32)
            for i in range(0, width, 128):
                square = square + floats[:, i : i + 128] * floats[:, i : i + 128]
            at = pl.ds(pl.multiple_of((tp ^ part) * width, width), width)
            rows[group * count : (group + 1) * count, at] = (
                floats * gain_ref[tp ^ part]
            ).astype(bf16)
        mean = jnp.sum(square, axis=-1, keepdims=True) * (1.0 / rows.shape[1])
        factors.append(lax.rsqrt(mean + eps))
    factor = jnp.concatenate(factors, axis=0)
    g = jnp.dot(rows[...], gate_ref[0], preferred_element_type=f32) * factor
    u = jnp.dot(rows[...], up_ref[0], preferred_element_type=f32) * factor
    out[...] = (g / (1.0 + jnp.exp(-g)) * u).astype(bf16)


def down_kernel(parts, capacity, where_ref, w_ref, *refs):
    pieces, (own_out, other_out, rows) = refs[:parts], refs[-3:]
    tp = where_ref[2]
    width = rows.shape[1] // parts
    for part in range(parts):
        rows[:, pl.ds(pl.multiple_of((tp ^ part) * width, width), width)] = pieces[part][...]
    total = jnp.dot(rows[...], w_ref[0], preferred_element_type=f32).astype(bf16)
    for i in range(total.shape[0] // capacity):
        at = i // 2 * capacity
        (own_out, other_out)[i % 2][at : at + capacity] = total[i * capacity : (i + 1) * capacity]


def combine_kernel(chips, count, capacity, routes, where_ref, *refs):
    ids_refs, mine_ref, theirs_ref = refs[:chips], refs[chips], refs[chips + 1]
    outs, rows = refs[chips + 2 : 2 * chips + 2], refs[-1]
    chip, core = where_ref[0], where_ref[1]
    before = (
        lax.broadcasted_iota(jnp.int32, (count, count), 0)
        < lax.broadcasted_iota(jnp.int32, (count, count), 1)
    ).astype(f32).astype(bf16)
    row_of = lax.broadcasted_iota(jnp.int32, (capacity, count), 0).astype(f32)
    for slot, out in enumerate(outs):
        part = ids_refs[slot][count : count + 8, 0:count].astype(f32)
        terms = [[], [], []]
        for side, results in ((0, mine_ref), (1, theirs_ref)):
            rows[side * capacity : (side + 1) * capacity] = results[
                slot * capacity : (slot + 1) * capacity
            ]
            expert = (2 * chip + (core ^ side)).astype(f32)
            chosen = jnp.zeros((1, count), f32)
            share = [jnp.zeros((1, count), f32)] * 3
            for k in range(routes):
                same = part[k : k + 1] == expert
                chosen = jnp.where(same, 1.0, chosen)
                for i in range(3):
                    at = routes * (1 + i) + k
                    share[i] = jnp.where(same, part[at : at + 1], share[i])
            rank = jnp.dot(
                jnp.broadcast_to(chosen, (8, count)).astype(bf16),
                before,
                preferred_element_type=f32,
            )[0:1]
            rank = jnp.where(chosen > 0, rank, -1.0)
            for i in range(3):
                terms[i].append(jnp.where(row_of == rank, share[i], 0.0).astype(bf16))
        total = jnp.zeros(out.shape, f32)
        for i in range(3):
            total = total + lax.dot_general(
                jnp.concatenate(terms[i], axis=0),
                rows[...],
                (((0,), (0,)), ((), ())),
                preferred_element_type=f32,
            )
        out[...] = total.astype(bf16)


def per_device_fast(
    query_rows,
    key_rows,
    value_rows,
    second_scale,
    head_gain,
    out_weight,
    routed_rows,
    norm_gain,
    route_ids,
    route_weight,
    expert_gate,
    expert_up,
    expert_down,
):
    ep_devices, tp_devices = lax.axis_size("ep"), lax.axis_size("tp")
    chips = ep_devices // 2
    count_a, count_b = query_rows.shape[0], routed_rows.shape[0]
    heads_here = second_scale.shape[0]
    width = query_rows.shape[1] // heads_here
    columns = routed_rows.shape[1]
    model = columns * tp_devices
    routes = route_ids.shape[1]
    capacity = 2 * count_b * routes // ep_devices
    units = expert_gate.shape[2]
    out_columns = out_weight.shape[1]
    ep_at = lax.axis_index("ep")
    where = jnp.stack([ep_at // 2, ep_at % 2, lax.axis_index("tp")]).astype(jnp.int32)

    def over_ep(value, slot, cross=0):
        pairs = [(i, (((i // 2) ^ slot) * 2 + (i % 2)) ^ cross) for i in range(ep_devices)]
        return lax.ppermute(value, "ep", pairs)

    def over_tp(value, offset):
        return lax.ppermute(value, "tp", [(i, i ^ offset) for i in range(tp_devices)])

    def spread(value, first):
        second = 3 ^ first
        one = over_tp(value, first)
        two = over_tp(value, second)
        pieces = {0: value, first: one, second: two, 3: over_tp(one, second)}
        return [pieces[offset] for offset in range(tp_devices)]

    def spread_direct(value):
        return [value] + [over_tp(value, offset) for offset in range(1, tp_devices)]

    def call(body, out_shape, *args, scratch=(), scalars=1, limit=8, last=False):
        return pl.pallas_call(
            body,
            out_shape=out_shape if last else near_shapes(out_shape),
            in_specs=[smem] * scalars + [vmem] * (len(args) - scalars),
            out_specs=jax.tree.map(lambda _: vmem, out_shape),
            scratch_shapes=list(scratch),
            compiler_params=params(limit),
        )(*args[:scalars], *[near(arg) for arg in args[scalars:]])

    far = [
        pltpu.with_memory_space_constraint(value, pltpu.HBM)
        for value in (routed_rows, route_ids.T, route_weight.T)
    ]
    packed = pl.pallas_call(
        functools.partial(rows_kernel, count_b),
        out_shape=pltpu.VMEM((count_b + 4 * routes, columns), bf16),
        in_specs=[pl.BlockSpec(memory_space=pltpu.HBM)] * 3,
        out_specs=vmem,
        scratch_shapes=[
            pltpu.VMEM((routes, count_b), jnp.int32),
            pltpu.VMEM((routes, count_b), f32),
            pltpu.SemaphoreType.DMA((3,)),
        ],
        compiler_params=params(8),
    )(*far)
    arrived = [packed] + [over_ep(packed, slot) for slot in range(1, chips)]
    swapped = [over_ep(part, 0, 1) for part in arrived]

    packs = call(
        functools.partial(pack_kernel, width),
        [sds(count_a, 3 * width)] * chips,
        where,
        query_rows,
        key_rows,
        value_rows,
    )
    mine = [packs[0]] + [over_ep(packs[slot], slot) for slot in range(1, chips)]
    theirs = [over_ep(part, 0, 1) for part in mine]

    gain_parts = norm_gain.reshape(tp_devices, 1, columns)
    mixes = {}
    for slots in row_groups:
        total = 2 * capacity * len(slots)
        pieces = []
        for slot in slots:
            picked = call(
        functools.partial(select_kernel, count_b, routes, capacity, [(slot,)]),
        sds(2 * capacity, columns),
        where,
        arrived[slot],
        swapped[slot],
            )
            pieces += spread(picked, 1 + slot % 2)
        hidden = call(
            functools.partial(gate_up_kernel, tp_devices, len(slots)),
            sds(total, units),
            where,
            gain_parts,
            expert_gate,
            expert_up,
            *pieces,
            scratch=[pltpu.VMEM((total, model), bf16)],
            limit=16,
        )
        own_side, other_side = call(
            functools.partial(down_kernel, tp_devices, capacity),
            [sds(capacity * len(slots), columns)] * 2,
            where,
            expert_down,
            *spread_direct(hidden),
            scratch=[pltpu.VMEM((total, units * tp_devices), bf16)],
            limit=12,
        )
        mixed = call(
        functools.partial(combine_kernel, len(slots), count_b, capacity, routes),
        [sds(count_b, columns)] * len(slots),
        where,
        *[arrived[slot] for slot in slots],
        own_side,
        over_ep(other_side, 0, 1),
        scratch=[pltpu.VMEM((2 * capacity, columns), bf16)],
        )
        for slot, part in zip(slots, mixed):
            mixes[slot] = over_ep(part, slot) if slot else part

    head_outs = call(
        functools.partial(attention_kernel, chips, count_a, width),
        [sds(count_a, width)] * chips,
        where,
        second_scale,
        head_gain.reshape(1, width),
        *mine,
        *theirs,
        scalars=2,
        limit=24,
        scratch=[
            pltpu.VMEM((chips, 2 * count_a, width), bf16),
            pltpu.VMEM((chips, 2 * count_a, width), bf16),
            pltpu.VMEM((2 * count_a, width), bf16),
            pltpu.VMEM((chips, 2 * count_a, 2 * count_a), f32),
            pltpu.VMEM((2 * count_a, width), f32),
            pltpu.VMEM((2 * count_a, width), f32),
            pltpu.VMEM((2 * count_a, width), f32),
        ],
    )
    back = [head_outs[0]] + [over_ep(head_outs[slot], slot) for slot in range(1, chips)]
    pieces = []
    for number, group in enumerate(head_groups):
        value = jnp.concatenate([back[slot] for slot in group], axis=1)
        pieces += spread(value, 1 + number)
    mixer_out = call(
        functools.partial(project_kernel, tp_devices, head_groups, width),
        sds(count_a, out_columns),
        where,
        out_weight,
        *pieces,
        scratch=[pltpu.VMEM((count_a, out_weight.shape[0]), bf16)],
        limit=12,
        last=True,
    )
    expert_mix = functools.reduce(
        jnp.add, [mixes[slot].astype(f32) for slot in range(chips)]
    ).astype(bf16)
    return (mixer_out, expert_mix)


row_groups = [(0, 1), (2, 3)]
head_groups = [(0, 1), (2, 3)]


def fast_fits(mesh):
    return mesh.shape["tp"] == 4 and mesh.shape["ep"] == 8


def solution(mesh):
    placed = (
        P("ep", "tp"),
        P("ep", "tp"),
        P("ep", "tp"),
        P("tp"),
        P(),
        P(None, "tp"),
        P("ep", "tp"),
        P(),
        P("ep", None),
        P("ep", None),
        P("ep", None, "tp"),
        P("ep", None, "tp"),
        P("ep", None, "tp"),
    )
    fast = fast_fits(mesh)

    def body(*args):
        if not fast:
            return per_device(*args)
        return per_device_fast(*args)

    return jax.shard_map(
        body,
        mesh=mesh,
        in_specs=placed,
        out_specs=(P("ep", "tp"), P("ep", "tp")),
        check_vma=False,
    )
```

```python
import functools

import jax
import jax.numpy as jnp
from jax import lax
from jax.experimental import pallas as pl
from jax.experimental.pallas import tpu as pltpu
from jax.sharding import PartitionSpec as P


eps = 1e-06
head_factor = 0.8
neg_big = -1e30
key_block_rows = 1024


def rms_rows(rows_in, gain):
    floats = rows_in.astype(jnp.float32)
    factor = lax.rsqrt(jnp.mean(floats * floats, axis=-1, keepdims=True) + eps)
    return (floats * factor * gain).astype(jnp.bfloat16)


def per_device(
    query_rows,
    key_rows,
    value_rows,
    second_scale,
    head_gain,
    out_weight,
    routed_rows,
    norm_gain,
    route_ids,
    route_weight,
    expert_gate,
    expert_up,
    expert_down,
):
    count_a = query_rows.shape[0]
    per_head = second_scale.shape[0]
    head_dim = query_rows.shape[1] // (2 * per_head)
    value_dim = head_gain.shape[0]
    query_four = query_rows.reshape(count_a, per_head, 2, head_dim)
    query_pos = lax.axis_index("ep") * count_a + jnp.arange(count_a, dtype=jnp.int32)

    def key_block(carry_state, key_part, value_part, block_start):
        key_count = key_part.shape[0]
        key_four = key_part.reshape(key_count, per_head, 2, head_dim)
        value_three = value_part.reshape(key_count, per_head, value_dim)
        scores = jnp.einsum(
            "ihcd,jhcd->ihcj", query_four, key_four, preferred_element_type=jnp.float32
        ) * head_dim ** (-0.5)
        allowed = (
            query_pos[:, None] >= block_start + jnp.arange(key_count, dtype=jnp.int32)[None, :]
        )[:, None, None, :]
        scores = jnp.where(allowed, scores, neg_big)
        old_max, old_sum, old_acc = carry_state
        new_max = jnp.maximum(old_max, jnp.max(scores, axis=-1))
        weights = jnp.where(allowed, jnp.exp(scores - new_max[..., None]), 0.0)
        shrink = jnp.exp(old_max - new_max)
        new_sum = old_sum * shrink + jnp.sum(weights, axis=-1)
        update = jnp.einsum(
            "ihcj,jhe->ihce",
            weights.astype(jnp.bfloat16),
            value_three,
            preferred_element_type=jnp.float32,
        )
        return (new_max, new_sum, old_acc * shrink[..., None] + update)

    start_state = (
        jnp.full((count_a, per_head, 2), neg_big, jnp.float32),
        jnp.zeros((count_a, per_head, 2), jnp.float32),
        jnp.zeros((count_a, per_head, 2, value_dim), jnp.float32),
    )
    key_part = lax.all_gather(key_rows, "ep", axis=0, tiled=True)
    value_part = lax.all_gather(value_rows, "ep", axis=0, tiled=True)
    key_count = key_part.shape[0]

    def step_block(block_num, inner_state):
        offset_rows = block_num * key_block_rows
        key_slice = lax.dynamic_slice_in_dim(key_part, offset_rows, key_block_rows, 0)
        value_slice = lax.dynamic_slice_in_dim(value_part, offset_rows, key_block_rows, 0)
        return key_block(inner_state, key_slice, value_slice, offset_rows)

    _, run_sum, run_acc = lax.fori_loop(0, key_count // key_block_rows, step_block, start_state)
    maps_both = run_acc / run_sum[..., None]
    mixed_maps = maps_both[:, :, 0] - second_scale[None, :, None] * maps_both[:, :, 1]
    mean_sq = jnp.mean(mixed_maps * mixed_maps, axis=-1, keepdims=True)
    head_out = (
        (mixed_maps * lax.rsqrt(mean_sq + eps) * head_gain * head_factor)
        .astype(jnp.bfloat16)
        .reshape(count_a, per_head * value_dim)
    )
    count_b = routed_rows.shape[0]
    route_count = route_ids.shape[1]
    experts_here = expert_gate.shape[0]
    ep_devices = lax.axis_size("ep")
    expert_total = experts_here * ep_devices
    capacity = 2 * count_b * route_count // expert_total
    flat_expert = route_ids.reshape(-1)
    chosen = (flat_expert[:, None] == jnp.arange(expert_total, dtype=jnp.int32)[None, :]).astype(
        jnp.int32
    )
    ranks = jnp.sum((jnp.cumsum(chosen, axis=0) - 1) * chosen, axis=1)
    slot_of = flat_expert * capacity + ranks
    token_of = jnp.arange(count_b * route_count, dtype=jnp.int32) // route_count
    slot_token = jnp.full((expert_total * capacity,), count_b, jnp.int32).at[slot_of].set(token_of)
    padded = jnp.concatenate(
        [routed_rows, jnp.zeros((1, routed_rows.shape[1]), jnp.bfloat16)], axis=0
    )
    outgoing = padded[slot_token].reshape(ep_devices, experts_here, capacity, routed_rows.shape[1])
    column_parts = lax.all_to_all(outgoing, "ep", split_axis=0, concat_axis=0, tiled=True)
    arrived = rms_rows(lax.all_gather(column_parts, "tp", axis=3, tiled=True), norm_gain)
    gate_val = jnp.einsum(
        "sxcd,xdf->sxcf", arrived, expert_gate, preferred_element_type=jnp.float32
    )
    up_val = jnp.einsum("sxcd,xdf->sxcf", arrived, expert_up, preferred_element_type=jnp.float32)
    hidden = (jax.nn.silu(gate_val) * up_val).astype(jnp.bfloat16)
    weight_rows = out_weight
    attn_total = jnp.dot(
        lax.all_gather(
            head_out.reshape(1, 1, count_a, head_out.shape[1]), "tp", axis=3, tiled=True
        )[0, 0],
        weight_rows,
        preferred_element_type=jnp.float32,
    )
    weight_rows = expert_down
    moe_total = jnp.einsum(
        "sxcf,xfd->sxcd",
        lax.all_gather(hidden, "tp", axis=3, tiled=True),
        weight_rows,
        preferred_element_type=jnp.float32,
    )
    mixer_out = attn_total.astype(jnp.bfloat16)
    returned = lax.all_to_all(
        moe_total.astype(jnp.bfloat16), "ep", split_axis=0, concat_axis=0, tiled=True
    )
    flat_back = returned.reshape(expert_total * capacity, returned.shape[3])
    picked = flat_back[slot_of].astype(jnp.float32).reshape(count_b, route_count, returned.shape[3])
    expert_mix = jnp.sum(picked * route_weight[:, :, None], axis=1).astype(jnp.bfloat16)
    return (mixer_out, expert_mix)


bf16 = jnp.bfloat16
f32 = jnp.float32
vmem = pl.BlockSpec(memory_space=pltpu.VMEM)
smem = pl.BlockSpec(memory_space=pltpu.SMEM)


def params(limit):
    return pltpu.CompilerParams(vmem_limit_bytes=limit * 1024 * 1024)


def near_shapes(tree):
    return jax.tree.map(lambda leaf: pltpu.VMEM(leaf.shape, leaf.dtype), tree)


def sds(*shape):
    return jax.ShapeDtypeStruct(shape, bf16)


def pack_kernel(width, where_ref, q_ref, k_ref, v_ref, _, *refs):
    outs, (queries, sems) = refs[:-2], refs[-2:]
    chip = where_ref[0]
    scale = (width // 2) ** (-0.5)
    heads = [pl.ds(pl.multiple_of((chip ^ slot) * width, width), width) for slot in range(len(outs))]
    copies = [pltpu.make_async_copy(q_ref, queries, sems.at[0])]
    for slot, out in enumerate(outs):
        for i, ref in ((1, k_ref), (2, v_ref)):
            at = out.at[:, i * width : (i + 1) * width]
            sem = sems.at[2 * slot + i]
            copies.append(pltpu.make_async_copy(ref.at[:, heads[slot]], at, sem))
    for copy in copies:
        copy.start()
    copies[0].wait()
    for slot, out in enumerate(outs):
        out[:, 0:width] = (queries[:, heads[slot]].astype(f32) * scale).astype(bf16)
    for copy in copies[1:]:
        copy.wait()


def attention_kernel(chips, count, width, where_ref, scale_ref, gain_ref, *refs):
    own, other = refs[:chips], refs[chips : 2 * chips]
    outs = refs[2 * chips : 3 * chips]
    keys, values, queries, scores, acc, row_max, row_sum = refs[3 * chips :]
    chip, core = where_ref[0], where_ref[1]
    half = width // 2
    pair = 2 * count
    for slot in range(chips):
        at = chip ^ slot
        for parity, part in ((core, own[slot]), (1 - core, other[slot])):
            rows = pl.ds(pl.multiple_of(parity * count, count), count)
            keys[at, rows] = part[:, width : 2 * width]
            values[at, rows] = part[:, 2 * width : 3 * width]
    lane = lax.broadcasted_iota(jnp.int32, (count, width), 1)

    def widest(block):
        best = block[:, 0:width]
        for i in range(width, pair, width):
            best = jnp.maximum(best, block[:, i : i + width])
        return best

    def products(number):
        return lax.dot_general(
            queries[...], keys[number], (((1,), (1,)), ((), ())), preferred_element_type=f32
        )

    def weigh(number):
        top = row_max[...]
        block = [
            jnp.exp(scores[number, :, i : i + width] - top) for i in range(0, pair, width)
        ]
        total = functools.reduce(jnp.add, block)
        weights = jnp.concatenate([part.astype(bf16) for part in block], axis=1)
        return total, jnp.dot(weights, values[number], preferred_element_type=f32)

    for slot in range(chips):
        last = chip ^ slot
        rows = own[slot][:, 0:width]
        queries[0:count] = jnp.where(lane < half, rows, jnp.zeros_like(rows))
        queries[count:pair] = jnp.where(lane < half, jnp.zeros_like(rows), rows)
        allowed = lax.broadcasted_iota(jnp.int32, (pair, pair), 1) <= (
            lax.broadcasted_iota(jnp.int32, (pair, pair), 0) % count + core * count
        )
        masked = jnp.where(allowed, products(last), neg_big)
        scores[last] = masked
        row_max[...] = widest(masked)

        @pl.loop(0, last)
        def _(number):
            block = products(number)
            scores[number] = block
            row_max[...] = jnp.maximum(row_max[...], widest(block))

        row_max[...] = jnp.broadcast_to(
            jnp.max(row_max[...], axis=-1, keepdims=True), row_max.shape
        )
        row_sum[...], acc[...] = weigh(last)

        @pl.loop(0, last)
        def _(number):
            total, update = weigh(number)
            row_sum[...] += total
            acc[...] += update

        maps = acc[...] / jnp.sum(row_sum[...], axis=-1, keepdims=True)
        mixed = maps[0:count] - scale_ref[chip] * maps[count:pair]
        mean_sq = jnp.mean(mixed * mixed, axis=-1, keepdims=True)
        outs[slot][...] = (
            mixed * lax.rsqrt(mean_sq + eps) * gain_ref[...] * head_factor
        ).astype(bf16)


def fetch_kernel(value_ref, out):
    out[...] = value_ref[0, 0:8, 0:128]


def project_kernel(parts, groups, width, where_ref, w_ref, *refs):
    pieces, (out, heads) = refs[: len(groups) * parts], refs[-2:]
    chip, tp = where_ref[0], where_ref[2]
    depth = heads.shape[1] // parts
    for part in range(parts):
        for number, slots in enumerate(groups):
            for i, slot in enumerate(slots):
                at = pl.multiple_of((tp ^ part) * depth + (chip ^ slot) * width, width)
                heads[:, pl.ds(at, width)] = pieces[number * parts + part][
                    :, i * width : (i + 1) * width
                ]
    out[...] = jnp.dot(heads[...], w_ref[...], preferred_element_type=f32).astype(bf16)


def rows_kernel(count, rows_ref, ids_ref, share_ref, out, ids, share, sems):
    copies = [
        pltpu.make_async_copy(rows_ref, out.at[0:count], sems.at[0]),
        pltpu.make_async_copy(ids_ref, ids, sems.at[1]),
        pltpu.make_async_copy(share_ref, share, sems.at[2]),
    ]
    for copy in copies:
        copy.start()
    out[count:] = jnp.zeros((out.shape[0] - count, out.shape[1]), bf16)
    copies[1].wait()
    copies[2].wait()
    table, rest = [ids[...].astype(f32)], share[...]
    for _ in range(3):
        table.append(rest.astype(bf16).astype(f32))
        rest = rest - table[-1]
    out[count:, 0:count] = jnp.concatenate(table, axis=0).astype(bf16)
    copies[0].wait()


def select_kernel(count, routes, capacity, groups, where_ref, *refs):
    slots = [slot for group in groups for slot in group]
    own, other, outs = refs[: len(slots)], refs[len(slots) : 2 * len(slots)], refs[2 * len(slots) :]
    expert = (2 * where_ref[0] + where_ref[1]).astype(f32)
    before = (
        lax.broadcasted_iota(jnp.int32, (count, count), 0)
        < lax.broadcasted_iota(jnp.int32, (count, count), 1)
    ).astype(f32).astype(bf16)
    row_of = lax.broadcasted_iota(jnp.int32, (capacity, count), 0).astype(f32)
    at = 0
    for out, group in zip(outs, groups):
        for i in range(len(group)):
            for side, part in ((0, own[at]), (1, other[at])):
                ids = part[count : count + 8, 0:count].astype(f32)
                chosen = jnp.zeros((1, count), f32)
                for k in range(routes):
                    chosen = jnp.where(ids[k : k + 1] == expert, 1.0, chosen)
                rank = jnp.dot(
                    jnp.broadcast_to(chosen, (8, count)).astype(bf16),
                    before,
                    preferred_element_type=f32,
                )[0:1]
                rank = jnp.where(chosen > 0, rank, -1.0)
                pick = jnp.where(row_of == rank, 1.0, 0.0).astype(bf16)
                first = (2 * i + side) * capacity
                out[first : first + capacity] = jnp.dot(
                    pick, part[0:count], preferred_element_type=f32
                ).astype(bf16)
            at += 1


def gate_up_kernel(parts, groups, where_ref, gain_ref, gate_ref, up_ref, *refs):
    pieces, (out, rows) = refs[: groups * parts], refs[-2:]
    tp = where_ref[2]
    width = rows.shape[1] // parts
    count = rows.shape[0] // groups
    factors = []
    for group in range(groups):
        square = jnp.zeros((count, 128), f32)
        for part in range(parts):
            floats = pieces[group * parts + part][...].astype(f32)
            for i in range(0, width, 128):
                square = square + floats[:, i : i + 128] * floats[:, i : i + 128]
            at = pl.ds(pl.multiple_of((tp ^ part) * width, width), width)
            rows[group * count : (group + 1) * count, at] = (
                floats * gain_ref[tp ^ part]
            ).astype(bf16)
        mean = jnp.sum(square, axis=-1, keepdims=True) * (1.0 / rows.shape[1])
        factors.append(lax.rsqrt(mean + eps))
    factor = jnp.concatenate(factors, axis=0)
    g = jnp.dot(rows[...], gate_ref[0], preferred_element_type=f32) * factor
    u = jnp.dot(rows[...], up_ref[0], preferred_element_type=f32) * factor
    out[...] = (g / (1.0 + jnp.exp(-g)) * u).astype(bf16)


def down_kernel(parts, capacity, where_ref, w_ref, *refs):
    pieces, (own_out, other_out, rows) = refs[:parts], refs[-3:]
    tp = where_ref[2]
    width = rows.shape[1] // parts
    for part in range(parts):
        rows[:, pl.ds(pl.multiple_of((tp ^ part) * width, width), width)] = pieces[part][...]
    total = jnp.dot(rows[...], w_ref[0], preferred_element_type=f32).astype(bf16)
    for i in range(total.shape[0] // capacity):
        at = i // 2 * capacity
        (own_out, other_out)[i % 2][at : at + capacity] = total[i * capacity : (i + 1) * capacity]


def combine_kernel(chips, count, capacity, routes, where_ref, *refs):
    ids_refs, mine_ref, theirs_ref = refs[:chips], refs[chips], refs[chips + 1]
    outs, rows = refs[chips + 2 : 2 * chips + 2], refs[-1]
    chip, core = where_ref[0], where_ref[1]
    before = (
        lax.broadcasted_iota(jnp.int32, (count, count), 0)
        < lax.broadcasted_iota(jnp.int32, (count, count), 1)
    ).astype(f32).astype(bf16)
    row_of = lax.broadcasted_iota(jnp.int32, (capacity, count), 0).astype(f32)
    for slot, out in enumerate(outs):
        part = ids_refs[slot][count : count + 8, 0:count].astype(f32)
        terms = [[], [], []]
        for side, results in ((0, mine_ref), (1, theirs_ref)):
            rows[side * capacity : (side + 1) * capacity] = results[
                slot * capacity : (slot + 1) * capacity
            ]
            expert = (2 * chip + (core ^ side)).astype(f32)
            chosen = jnp.zeros((1, count), f32)
            share = [jnp.zeros((1, count), f32)] * 3
            for k in range(routes):
                same = part[k : k + 1] == expert
                chosen = jnp.where(same, 1.0, chosen)
                for i in range(3):
                    at = routes * (1 + i) + k
                    share[i] = jnp.where(same, part[at : at + 1], share[i])
            rank = jnp.dot(
                jnp.broadcast_to(chosen, (8, count)).astype(bf16),
                before,
                preferred_element_type=f32,
            )[0:1]
            rank = jnp.where(chosen > 0, rank, -1.0)
            for i in range(3):
                terms[i].append(jnp.where(row_of == rank, share[i], 0.0).astype(bf16))
        total = jnp.zeros(out.shape, f32)
        for i in range(3):
            total = total + lax.dot_general(
                jnp.concatenate(terms[i], axis=0),
                rows[...],
                (((0,), (0,)), ((), ())),
                preferred_element_type=f32,
            )
        out[...] = total.astype(bf16)


def per_device_fast(
    query_rows,
    key_rows,
    value_rows,
    second_scale,
    head_gain,
    out_weight,
    routed_rows,
    norm_gain,
    route_ids,
    route_weight,
    expert_gate,
    expert_up,
    expert_down,
):
    ep_devices, tp_devices = lax.axis_size("ep"), lax.axis_size("tp")
    chips = ep_devices // 2
    count_a, count_b = query_rows.shape[0], routed_rows.shape[0]
    heads_here = second_scale.shape[0]
    width = query_rows.shape[1] // heads_here
    columns = routed_rows.shape[1]
    model = columns * tp_devices
    routes = route_ids.shape[1]
    capacity = 2 * count_b * routes // ep_devices
    units = expert_gate.shape[2]
    out_columns = out_weight.shape[1]
    ep_at = lax.axis_index("ep")
    where = jnp.stack([ep_at // 2, ep_at % 2, lax.axis_index("tp")]).astype(jnp.int32)

    def over_ep(value, slot, cross=0):
        pairs = [(i, (((i // 2) ^ slot) * 2 + (i % 2)) ^ cross) for i in range(ep_devices)]
        return lax.ppermute(value, "ep", pairs)

    def over_tp(value, offset):
        return lax.ppermute(value, "tp", [(i, i ^ offset) for i in range(tp_devices)])

    def spread(value, first):
        second = 3 ^ first
        one = over_tp(value, first)
        two = over_tp(value, second)
        pieces = {0: value, first: one, second: two, 3: over_tp(one, second)}
        return [pieces[offset] for offset in range(tp_devices)]

    def spread_direct(value):
        return [value] + [over_tp(value, offset) for offset in range(1, tp_devices)]

    def call(body, out_shape, *args, scratch=(), scalars=1, limit=8, last=False, far=()):
        far_spec = pl.BlockSpec(memory_space=pltpu.HBM)
        specs = [vmem if i not in far else far_spec for i in range(len(args) - scalars)]
        placed = [
            pltpu.with_memory_space_constraint(value, pltpu.HBM if i in far else pltpu.VMEM)
            for i, value in enumerate(args[scalars:])
        ]
        return pl.pallas_call(
            body,
            out_shape=out_shape if last else near_shapes(out_shape),
            in_specs=[smem] * scalars + specs,
            out_specs=jax.tree.map(lambda _: vmem, out_shape),
            scratch_shapes=list(scratch),
            compiler_params=params(limit),
        )(*args[:scalars], *placed)

    far = [
        pltpu.with_memory_space_constraint(value, pltpu.HBM)
        for value in (routed_rows, route_ids.T, route_weight.T)
    ]
    packed = pl.pallas_call(
        functools.partial(rows_kernel, count_b),
        out_shape=pltpu.VMEM((count_b + 4 * routes, columns), bf16),
        in_specs=[pl.BlockSpec(memory_space=pltpu.HBM)] * 3,
        out_specs=vmem,
        scratch_shapes=[
            pltpu.VMEM((routes, count_b), jnp.int32),
            pltpu.VMEM((routes, count_b), f32),
            pltpu.SemaphoreType.DMA((3,)),
        ],
        compiler_params=params(8),
    )(*far)
    arrived = [packed] + [over_ep(packed, slot) for slot in range(1, chips)]
    swapped = [over_ep(part, 0, 1) for part in arrived]

    fetched = [
        call(fetch_kernel, sds(8, 128), value, scalars=0)
        for value in (expert_gate, expert_up)
    ]

    packs = pl.pallas_call(
        functools.partial(pack_kernel, width),
        out_shape=[pltpu.VMEM((count_a, 3 * width), bf16)] * chips,
        in_specs=[smem] + [pl.BlockSpec(memory_space=pltpu.HBM)] * 3 + [vmem],
        out_specs=[vmem] * chips,
        scratch_shapes=[
            pltpu.VMEM(query_rows.shape, bf16),
            pltpu.SemaphoreType.DMA((2 * chips + 1,)),
        ],
        compiler_params=params(8),
    )(
        where,
        *[
            pltpu.with_memory_space_constraint(value, pltpu.HBM)
            for value in (query_rows, key_rows, value_rows)
        ],
        fetched[0],
    )
    mine = [packs[0]] + [over_ep(packs[slot], slot) for slot in range(1, chips)]
    theirs = [over_ep(part, 0, 1) for part in mine]

    gain_parts = norm_gain.reshape(tp_devices, 1, columns)
    mixes = {}
    for slots in row_groups:
        total = 2 * capacity * len(slots)
        pieces = []
        for slot in slots:
            picked = call(
        functools.partial(select_kernel, count_b, routes, capacity, [(slot,)]),
        sds(2 * capacity, columns),
        where,
        arrived[slot],
        swapped[slot],
            )
            pieces += spread(picked, 1 + slot % 2)
        hidden = call(
            functools.partial(gate_up_kernel, tp_devices, len(slots)),
            sds(total, units),
            where,
            gain_parts,
            expert_gate,
            expert_up,
            *pieces,
            fetched[1],
            scratch=[pltpu.VMEM((total, model), bf16)],
            limit=16,
        )
        own_side, other_side = call(
            functools.partial(down_kernel, tp_devices, capacity),
            [sds(capacity * len(slots), columns)] * 2,
            where,
            expert_down,
            *spread_direct(hidden),
            scratch=[pltpu.VMEM((total, units * tp_devices), bf16)],
            limit=12,
        )
        mixed = call(
        functools.partial(combine_kernel, len(slots), count_b, capacity, routes),
        [sds(count_b, columns)] * len(slots),
        where,
        *[arrived[slot] for slot in slots],
        own_side,
        over_ep(other_side, 0, 1),
        scratch=[pltpu.VMEM((2 * capacity, columns), bf16)],
        )
        for slot, part in zip(slots, mixed):
            mixes[slot] = over_ep(part, slot) if slot else part

    head_outs = call(
        functools.partial(attention_kernel, chips, count_a, width),
        [sds(count_a, width)] * chips,
        where,
        second_scale,
        head_gain.reshape(1, width),
        *mine,
        *theirs,
        scalars=2,
        limit=24,
        scratch=[
            pltpu.VMEM((chips, 2 * count_a, width), bf16),
            pltpu.VMEM((chips, 2 * count_a, width), bf16),
            pltpu.VMEM((2 * count_a, width), bf16),
            pltpu.VMEM((chips, 2 * count_a, 2 * count_a), f32),
            pltpu.VMEM((2 * count_a, width), f32),
            pltpu.VMEM((2 * count_a, width), f32),
            pltpu.VMEM((2 * count_a, width), f32),
        ],
    )
    back = [head_outs[0]] + [over_ep(head_outs[slot], slot) for slot in range(1, chips)]
    pieces = []
    for number, group in enumerate(head_groups):
        value = jnp.concatenate([back[slot] for slot in group], axis=1)
        pieces += spread(value, 1 + number)
    mixer_out = call(
        functools.partial(project_kernel, tp_devices, head_groups, width),
        sds(count_a, out_columns),
        where,
        out_weight,
        *pieces,
        scratch=[pltpu.VMEM((count_a, out_weight.shape[0]), bf16)],
        limit=12,
        last=True,
    )
    expert_mix = functools.reduce(
        jnp.add, [mixes[slot].astype(f32) for slot in range(chips)]
    ).astype(bf16)
    return (mixer_out, expert_mix)


row_groups = [(0, 1), (2, 3)]
head_groups = [(0, 1), (2, 3)]


def fast_fits(mesh):
    return mesh.shape["tp"] == 4 and mesh.shape["ep"] == 8


def solution(mesh):
    placed = (
        P("ep", "tp"),
        P("ep", "tp"),
        P("ep", "tp"),
        P("tp"),
        P(),
        P(None, "tp"),
        P("ep", "tp"),
        P(),
        P("ep", None),
        P("ep", None),
        P("ep", None, "tp"),
        P("ep", None, "tp"),
        P("ep", None, "tp"),
    )
    fast = fast_fits(mesh)

    def body(*args):
        if not fast:
            return per_device(*args)
        return per_device_fast(*args)

    return jax.shard_map(
        body,
        mesh=mesh,
        in_specs=placed,
        out_specs=(P("ep", "tp"), P("ep", "tp")),
        check_vma=False,
    )
```

```python
import functools

import jax
import jax.numpy as jnp
from jax import lax
from jax.experimental import pallas as pl
from jax.experimental.pallas import tpu as pltpu
from jax.sharding import PartitionSpec as P


eps = 1e-06
head_factor = 0.8
neg_big = -1e30
key_block_rows = 1024


def rms_rows(rows_in, gain):
    floats = rows_in.astype(jnp.float32)
    factor = lax.rsqrt(jnp.mean(floats * floats, axis=-1, keepdims=True) + eps)
    return (floats * factor * gain).astype(jnp.bfloat16)


def per_device(
    query_rows,
    key_rows,
    value_rows,
    second_scale,
    head_gain,
    out_weight,
    routed_rows,
    norm_gain,
    route_ids,
    route_weight,
    expert_gate,
    expert_up,
    expert_down,
):
    count_a = query_rows.shape[0]
    per_head = second_scale.shape[0]
    head_dim = query_rows.shape[1] // (2 * per_head)
    value_dim = head_gain.shape[0]
    query_four = query_rows.reshape(count_a, per_head, 2, head_dim)
    query_pos = lax.axis_index("ep") * count_a + jnp.arange(count_a, dtype=jnp.int32)

    def key_block(carry_state, key_part, value_part, block_start):
        key_count = key_part.shape[0]
        key_four = key_part.reshape(key_count, per_head, 2, head_dim)
        value_three = value_part.reshape(key_count, per_head, value_dim)
        scores = jnp.einsum(
            "ihcd,jhcd->ihcj", query_four, key_four, preferred_element_type=jnp.float32
        ) * head_dim ** (-0.5)
        allowed = (
            query_pos[:, None] >= block_start + jnp.arange(key_count, dtype=jnp.int32)[None, :]
        )[:, None, None, :]
        scores = jnp.where(allowed, scores, neg_big)
        old_max, old_sum, old_acc = carry_state
        new_max = jnp.maximum(old_max, jnp.max(scores, axis=-1))
        weights = jnp.where(allowed, jnp.exp(scores - new_max[..., None]), 0.0)
        shrink = jnp.exp(old_max - new_max)
        new_sum = old_sum * shrink + jnp.sum(weights, axis=-1)
        update = jnp.einsum(
            "ihcj,jhe->ihce",
            weights.astype(jnp.bfloat16),
            value_three,
            preferred_element_type=jnp.float32,
        )
        return (new_max, new_sum, old_acc * shrink[..., None] + update)

    start_state = (
        jnp.full((count_a, per_head, 2), neg_big, jnp.float32),
        jnp.zeros((count_a, per_head, 2), jnp.float32),
        jnp.zeros((count_a, per_head, 2, value_dim), jnp.float32),
    )
    key_part = lax.all_gather(key_rows, "ep", axis=0, tiled=True)
    value_part = lax.all_gather(value_rows, "ep", axis=0, tiled=True)
    key_count = key_part.shape[0]

    def step_block(block_num, inner_state):
        offset_rows = block_num * key_block_rows
        key_slice = lax.dynamic_slice_in_dim(key_part, offset_rows, key_block_rows, 0)
        value_slice = lax.dynamic_slice_in_dim(value_part, offset_rows, key_block_rows, 0)
        return key_block(inner_state, key_slice, value_slice, offset_rows)

    _, run_sum, run_acc = lax.fori_loop(0, key_count // key_block_rows, step_block, start_state)
    maps_both = run_acc / run_sum[..., None]
    mixed_maps = maps_both[:, :, 0] - second_scale[None, :, None] * maps_both[:, :, 1]
    mean_sq = jnp.mean(mixed_maps * mixed_maps, axis=-1, keepdims=True)
    head_out = (
        (mixed_maps * lax.rsqrt(mean_sq + eps) * head_gain * head_factor)
        .astype(jnp.bfloat16)
        .reshape(count_a, per_head * value_dim)
    )
    count_b = routed_rows.shape[0]
    route_count = route_ids.shape[1]
    experts_here = expert_gate.shape[0]
    ep_devices = lax.axis_size("ep")
    expert_total = experts_here * ep_devices
    capacity = 2 * count_b * route_count // expert_total
    flat_expert = route_ids.reshape(-1)
    chosen = (flat_expert[:, None] == jnp.arange(expert_total, dtype=jnp.int32)[None, :]).astype(
        jnp.int32
    )
    ranks = jnp.sum((jnp.cumsum(chosen, axis=0) - 1) * chosen, axis=1)
    slot_of = flat_expert * capacity + ranks
    token_of = jnp.arange(count_b * route_count, dtype=jnp.int32) // route_count
    slot_token = jnp.full((expert_total * capacity,), count_b, jnp.int32).at[slot_of].set(token_of)
    padded = jnp.concatenate(
        [routed_rows, jnp.zeros((1, routed_rows.shape[1]), jnp.bfloat16)], axis=0
    )
    outgoing = padded[slot_token].reshape(ep_devices, experts_here, capacity, routed_rows.shape[1])
    column_parts = lax.all_to_all(outgoing, "ep", split_axis=0, concat_axis=0, tiled=True)
    arrived = rms_rows(lax.all_gather(column_parts, "tp", axis=3, tiled=True), norm_gain)
    gate_val = jnp.einsum(
        "sxcd,xdf->sxcf", arrived, expert_gate, preferred_element_type=jnp.float32
    )
    up_val = jnp.einsum("sxcd,xdf->sxcf", arrived, expert_up, preferred_element_type=jnp.float32)
    hidden = (jax.nn.silu(gate_val) * up_val).astype(jnp.bfloat16)
    weight_rows = out_weight
    attn_total = jnp.dot(
        lax.all_gather(
            head_out.reshape(1, 1, count_a, head_out.shape[1]), "tp", axis=3, tiled=True
        )[0, 0],
        weight_rows,
        preferred_element_type=jnp.float32,
    )
    weight_rows = expert_down
    moe_total = jnp.einsum(
        "sxcf,xfd->sxcd",
        lax.all_gather(hidden, "tp", axis=3, tiled=True),
        weight_rows,
        preferred_element_type=jnp.float32,
    )
    mixer_out = attn_total.astype(jnp.bfloat16)
    returned = lax.all_to_all(
        moe_total.astype(jnp.bfloat16), "ep", split_axis=0, concat_axis=0, tiled=True
    )
    flat_back = returned.reshape(expert_total * capacity, returned.shape[3])
    picked = flat_back[slot_of].astype(jnp.float32).reshape(count_b, route_count, returned.shape[3])
    expert_mix = jnp.sum(picked * route_weight[:, :, None], axis=1).astype(jnp.bfloat16)
    return (mixer_out, expert_mix)


bf16 = jnp.bfloat16
f32 = jnp.float32
vmem = pl.BlockSpec(memory_space=pltpu.VMEM)
smem = pl.BlockSpec(memory_space=pltpu.SMEM)


def params(limit):
    return pltpu.CompilerParams(vmem_limit_bytes=limit * 1024 * 1024)


def near_shapes(tree):
    return jax.tree.map(lambda leaf: pltpu.VMEM(leaf.shape, leaf.dtype), tree)


def sds(*shape):
    return jax.ShapeDtypeStruct(shape, bf16)


def pack_kernel(width, where_ref, q_ref, k_ref, v_ref, _, *refs):
    outs, (queries, sems) = refs[:-2], refs[-2:]
    chip = where_ref[0]
    scale = (width // 2) ** (-0.5)
    heads = [pl.ds(pl.multiple_of((chip ^ slot) * width, width), width) for slot in range(len(outs))]
    copies = [pltpu.make_async_copy(q_ref, queries, sems.at[0])]
    for slot, out in enumerate(outs):
        for i, ref in ((1, k_ref), (2, v_ref)):
            at = out.at[:, i * width : (i + 1) * width]
            sem = sems.at[2 * slot + i]
            copies.append(pltpu.make_async_copy(ref.at[:, heads[slot]], at, sem))
    for copy in copies:
        copy.start()
    copies[0].wait()
    for slot, out in enumerate(outs):
        out[:, 0:width] = (queries[:, heads[slot]].astype(f32) * scale).astype(bf16)
    for copy in copies[1:]:
        copy.wait()


def fill_keys(chip, core, base, count, width, own, other, keys, values):
    for slot in range(len(own)):
        at = (chip ^ slot) - base
        for parity, part in ((core, own[slot]), (1 - core, other[slot])):
            rows = pl.ds(pl.multiple_of(parity * count, count), count)
            keys[at, rows] = part[:, width : 2 * width]
            values[at, rows] = part[:, 2 * width : 3 * width]


def softmax_rows(rows, keys, values, queries, scores, state, upto, core, start=None):
    acc, row_max, row_sum = state
    count, width = rows.shape
    half, pair = width // 2, 2 * count
    lane = lax.broadcasted_iota(jnp.int32, (count, width), 1)
    queries[0:count] = jnp.where(lane < half, rows, jnp.zeros_like(rows))
    queries[count:pair] = jnp.where(lane < half, jnp.zeros_like(rows), rows)

    def widest(block):
        best = block[:, 0:width]
        for i in range(width, pair, width):
            best = jnp.maximum(best, block[:, i : i + width])
        return best

    def products(number):
        return lax.dot_general(
            queries[...], keys[number], (((1,), (1,)), ((), ())), preferred_element_type=f32
        )

    def weigh(number):
        top = row_max[...]
        block = [jnp.exp(scores[number, :, i : i + width] - top) for i in range(0, pair, width)]
        total = functools.reduce(jnp.add, block)
        weights = jnp.concatenate([part.astype(bf16) for part in block], axis=1)
        return total, jnp.dot(weights, values[number], preferred_element_type=f32)

    if start is None:
        allowed = lax.broadcasted_iota(jnp.int32, (pair, pair), 1) <= (
            lax.broadcasted_iota(jnp.int32, (pair, pair), 0) % count + core * count
        )
        masked = jnp.where(allowed, products(upto), neg_big)
        scores[upto] = masked
        row_max[...] = widest(masked)
    else:
        row_max[...] = start[1][...]

    @pl.loop(0, upto)
    def _(number):
        block = products(number)
        scores[number] = block
        row_max[...] = jnp.maximum(row_max[...], widest(block))

    row_max[...] = jnp.broadcast_to(
        jnp.max(row_max[...], axis=-1, keepdims=True), row_max.shape
    )
    if start is None:
        row_sum[...], acc[...] = weigh(upto)
    else:
        shrink = jnp.exp(start[1][...] - row_max[...])
        acc[...] = start[0][...] * shrink
        row_sum[...] = start[2][...] * shrink

    @pl.loop(0, upto)
    def _(number):
        total, update = weigh(number)
        row_sum[...] += total
        acc[...] += update


def near_attention_kernel(count, width, where_ref, *refs):
    own, other, outs = refs[0:2], refs[2:4], refs[4:10]
    keys, values, queries, scores = refs[10:]
    chip, core = where_ref[0], where_ref[1]
    base = chip // 2 * 2
    fill_keys(chip, core, base, count, width, own, other, keys, values)
    for slot in range(2):
        state = outs[3 * slot : 3 * slot + 3]
        last = (chip ^ slot) - base
        rows = own[slot][:, 0:width]
        softmax_rows(rows, keys, values, queries, scores, state, last, core)


def attention_kernel(chips, count, width, where_ref, scale_ref, gain_ref, *refs):
    own, other = refs[:chips], refs[chips : 2 * chips]
    starts = refs[2 * chips : 2 * chips + 6]
    outs = refs[2 * chips + 6 : 3 * chips + 6]
    keys, values, queries, scores, acc, row_max, row_sum = refs[3 * chips + 6 :]
    chip, core = where_ref[0], where_ref[1]
    pair = 2 * count
    fill_keys(chip, core, 0, count, width, own, other, keys, values)
    for slot in range(chips):
        start = starts[3 * slot : 3 * slot + 3] if slot < 2 else None
        upto = chip // 2 * 2 if slot < 2 else chip ^ slot
        rows = own[slot][:, 0:width]
        state = (acc, row_max, row_sum)
        softmax_rows(rows, keys, values, queries, scores, state, upto, core, start)
        maps = acc[...] / jnp.sum(row_sum[...], axis=-1, keepdims=True)
        mixed = maps[0:count] - scale_ref[chip] * maps[count:pair]
        mean_sq = jnp.mean(mixed * mixed, axis=-1, keepdims=True)
        outs[slot][...] = (
            mixed * lax.rsqrt(mean_sq + eps) * gain_ref[...] * head_factor
        ).astype(bf16)


def fetch_kernel(value_ref, out):
    out[...] = value_ref[0, 0:8, 0:128]


def project_kernel(parts, groups, width, where_ref, w_ref, *refs):
    pieces, (out, heads) = refs[: len(groups) * parts], refs[-2:]
    chip, tp = where_ref[0], where_ref[2]
    depth = heads.shape[1] // parts
    for part in range(parts):
        for number, slots in enumerate(groups):
            for i, slot in enumerate(slots):
                at = pl.multiple_of((tp ^ part) * depth + (chip ^ slot) * width, width)
                heads[:, pl.ds(at, width)] = pieces[number * parts + part][
                    :, i * width : (i + 1) * width
                ]
    out[...] = jnp.dot(heads[...], w_ref[...], preferred_element_type=f32).astype(bf16)


def rows_kernel(count, rows_ref, ids_ref, share_ref, out, ids, share, sems):
    copies = [
        pltpu.make_async_copy(rows_ref, out.at[0:count], sems.at[0]),
        pltpu.make_async_copy(ids_ref, ids, sems.at[1]),
        pltpu.make_async_copy(share_ref, share, sems.at[2]),
    ]
    for copy in copies:
        copy.start()
    out[count:] = jnp.zeros((out.shape[0] - count, out.shape[1]), bf16)
    copies[1].wait()
    copies[2].wait()
    table, rest = [ids[...].astype(f32)], share[...]
    for _ in range(3):
        table.append(rest.astype(bf16).astype(f32))
        rest = rest - table[-1]
    out[count:, 0:count] = jnp.concatenate(table, axis=0).astype(bf16)
    copies[0].wait()


def select_kernel(count, routes, capacity, groups, where_ref, *refs):
    slots = [slot for group in groups for slot in group]
    own, other, outs = refs[: len(slots)], refs[len(slots) : 2 * len(slots)], refs[2 * len(slots) :]
    expert = (2 * where_ref[0] + where_ref[1]).astype(f32)
    before = (
        lax.broadcasted_iota(jnp.int32, (count, count), 0)
        < lax.broadcasted_iota(jnp.int32, (count, count), 1)
    ).astype(f32).astype(bf16)
    row_of = lax.broadcasted_iota(jnp.int32, (capacity, count), 0).astype(f32)
    at = 0
    for out, group in zip(outs, groups):
        for i in range(len(group)):
            for side, part in ((0, own[at]), (1, other[at])):
                ids = part[count : count + 8, 0:count].astype(f32)
                chosen = jnp.zeros((1, count), f32)
                for k in range(routes):
                    chosen = jnp.where(ids[k : k + 1] == expert, 1.0, chosen)
                rank = jnp.dot(
                    jnp.broadcast_to(chosen, (8, count)).astype(bf16),
                    before,
                    preferred_element_type=f32,
                )[0:1]
                rank = jnp.where(chosen > 0, rank, -1.0)
                pick = jnp.where(row_of == rank, 1.0, 0.0).astype(bf16)
                first = (2 * i + side) * capacity
                out[first : first + capacity] = jnp.dot(
                    pick, part[0:count], preferred_element_type=f32
                ).astype(bf16)
            at += 1


def gate_up_kernel(parts, groups, where_ref, gain_ref, gate_ref, up_ref, *refs):
    pieces, (out, rows) = refs[: groups * parts], refs[-2:]
    tp = where_ref[2]
    width = rows.shape[1] // parts
    count = rows.shape[0] // groups
    factors = []
    for group in range(groups):
        square = jnp.zeros((count, 128), f32)
        for part in range(parts):
            floats = pieces[group * parts + part][...].astype(f32)
            for i in range(0, width, 128):
                square = square + floats[:, i : i + 128] * floats[:, i : i + 128]
            at = pl.ds(pl.multiple_of((tp ^ part) * width, width), width)
            rows[group * count : (group + 1) * count, at] = (
                floats * gain_ref[tp ^ part]
            ).astype(bf16)
        mean = jnp.sum(square, axis=-1, keepdims=True) * (1.0 / rows.shape[1])
        factors.append(lax.rsqrt(mean + eps))
    factor = jnp.concatenate(factors, axis=0)
    g = jnp.dot(rows[...], gate_ref[0], preferred_element_type=f32) * factor
    u = jnp.dot(rows[...], up_ref[0], preferred_element_type=f32) * factor
    out[...] = (g / (1.0 + jnp.exp(-g)) * u).astype(bf16)


def down_kernel(parts, capacity, where_ref, w_ref, *refs):
    pieces, (own_out, other_out, rows) = refs[:parts], refs[-3:]
    tp = where_ref[2]
    width = rows.shape[1] // parts
    for part in range(parts):
        rows[:, pl.ds(pl.multiple_of((tp ^ part) * width, width), width)] = pieces[part][...]
    total = jnp.dot(rows[...], w_ref[0], preferred_element_type=f32).astype(bf16)
    for i in range(total.shape[0] // capacity):
        at = i // 2 * capacity
        (own_out, other_out)[i % 2][at : at + capacity] = total[i * capacity : (i + 1) * capacity]


def combine_kernel(chips, count, capacity, routes, where_ref, *refs):
    ids_refs, mine_ref, theirs_ref = refs[:chips], refs[chips], refs[chips + 1]
    outs, rows = refs[chips + 2 : 2 * chips + 2], refs[-1]
    chip, core = where_ref[0], where_ref[1]
    before = (
        lax.broadcasted_iota(jnp.int32, (count, count), 0)
        < lax.broadcasted_iota(jnp.int32, (count, count), 1)
    ).astype(f32).astype(bf16)
    row_of = lax.broadcasted_iota(jnp.int32, (capacity, count), 0).astype(f32)
    for slot, out in enumerate(outs):
        part = ids_refs[slot][count : count + 8, 0:count].astype(f32)
        terms = [[], [], []]
        for side, results in ((0, mine_ref), (1, theirs_ref)):
            rows[side * capacity : (side + 1) * capacity] = results[
                slot * capacity : (slot + 1) * capacity
            ]
            expert = (2 * chip + (core ^ side)).astype(f32)
            chosen = jnp.zeros((1, count), f32)
            share = [jnp.zeros((1, count), f32)] * 3
            for k in range(routes):
                same = part[k : k + 1] == expert
                chosen = jnp.where(same, 1.0, chosen)
                for i in range(3):
                    at = routes * (1 + i) + k
                    share[i] = jnp.where(same, part[at : at + 1], share[i])
            rank = jnp.dot(
                jnp.broadcast_to(chosen, (8, count)).astype(bf16),
                before,
                preferred_element_type=f32,
            )[0:1]
            rank = jnp.where(chosen > 0, rank, -1.0)
            for i in range(3):
                terms[i].append(jnp.where(row_of == rank, share[i], 0.0).astype(bf16))
        total = jnp.zeros(out.shape, f32)
        for i in range(3):
            total = total + lax.dot_general(
                jnp.concatenate(terms[i], axis=0),
                rows[...],
                (((0,), (0,)), ((), ())),
                preferred_element_type=f32,
            )
        out[...] = total.astype(bf16)


def per_device_fast(
    query_rows,
    key_rows,
    value_rows,
    second_scale,
    head_gain,
    out_weight,
    routed_rows,
    norm_gain,
    route_ids,
    route_weight,
    expert_gate,
    expert_up,
    expert_down,
):
    ep_devices, tp_devices = lax.axis_size("ep"), lax.axis_size("tp")
    chips = ep_devices // 2
    count_a, count_b = query_rows.shape[0], routed_rows.shape[0]
    heads_here = second_scale.shape[0]
    width = query_rows.shape[1] // heads_here
    columns = routed_rows.shape[1]
    model = columns * tp_devices
    routes = route_ids.shape[1]
    capacity = 2 * count_b * routes // ep_devices
    units = expert_gate.shape[2]
    out_columns = out_weight.shape[1]
    ep_at = lax.axis_index("ep")
    where = jnp.stack([ep_at // 2, ep_at % 2, lax.axis_index("tp")]).astype(jnp.int32)

    def over_ep(value, slot, cross=0):
        pairs = [(i, (((i // 2) ^ slot) * 2 + (i % 2)) ^ cross) for i in range(ep_devices)]
        return lax.ppermute(value, "ep", pairs)

    def over_tp(value, offset):
        return lax.ppermute(value, "tp", [(i, i ^ offset) for i in range(tp_devices)])

    def spread(value, first):
        second = 3 ^ first
        one = over_tp(value, first)
        two = over_tp(value, second)
        pieces = {0: value, first: one, second: two, 3: over_tp(one, second)}
        return [pieces[offset] for offset in range(tp_devices)]

    def spread_direct(value):
        return [value] + [over_tp(value, offset) for offset in range(1, tp_devices)]

    def call(body, out_shape, *args, scratch=(), scalars=1, limit=8, last=False, far=()):
        far_spec = pl.BlockSpec(memory_space=pltpu.HBM)
        specs = [vmem if i not in far else far_spec for i in range(len(args) - scalars)]
        placed = [
            pltpu.with_memory_space_constraint(value, pltpu.HBM if i in far else pltpu.VMEM)
            for i, value in enumerate(args[scalars:])
        ]
        return pl.pallas_call(
            body,
            out_shape=out_shape if last else near_shapes(out_shape),
            in_specs=[smem] * scalars + specs,
            out_specs=jax.tree.map(lambda _: vmem, out_shape),
            scratch_shapes=list(scratch),
            compiler_params=params(limit),
        )(*args[:scalars], *placed)

    far = [
        pltpu.with_memory_space_constraint(value, pltpu.HBM)
        for value in (routed_rows, route_ids.T, route_weight.T)
    ]
    packed = pl.pallas_call(
        functools.partial(rows_kernel, count_b),
        out_shape=pltpu.VMEM((count_b + 4 * routes, columns), bf16),
        in_specs=[pl.BlockSpec(memory_space=pltpu.HBM)] * 3,
        out_specs=vmem,
        scratch_shapes=[
            pltpu.VMEM((routes, count_b), jnp.int32),
            pltpu.VMEM((routes, count_b), f32),
            pltpu.SemaphoreType.DMA((3,)),
        ],
        compiler_params=params(8),
    )(*far)
    arrived = [packed] + [over_ep(packed, slot) for slot in range(1, chips)]
    swapped = [over_ep(part, 0, 1) for part in arrived]

    fetched = [
        call(fetch_kernel, sds(8, 128), value, scalars=0)
        for value in (expert_gate, expert_up)
    ]

    packs = pl.pallas_call(
        functools.partial(pack_kernel, width),
        out_shape=[pltpu.VMEM((count_a, 3 * width), bf16)] * chips,
        in_specs=[smem] + [pl.BlockSpec(memory_space=pltpu.HBM)] * 3 + [vmem],
        out_specs=[vmem] * chips,
        scratch_shapes=[
            pltpu.VMEM(query_rows.shape, bf16),
            pltpu.SemaphoreType.DMA((2 * chips + 1,)),
        ],
        compiler_params=params(8),
    )(
        where,
        *[
            pltpu.with_memory_space_constraint(value, pltpu.HBM)
            for value in (query_rows, key_rows, value_rows)
        ],
        fetched[0],
    )
    mine = [packs[0]] + [over_ep(packs[slot], slot) for slot in range(1, chips)]
    theirs = [over_ep(part, 0, 1) for part in mine]

    gain_parts = norm_gain.reshape(tp_devices, 1, columns)
    mixes = {}
    for slots in row_groups:
        total = 2 * capacity * len(slots)
        pieces = []
        for slot in slots:
            picked = call(
        functools.partial(select_kernel, count_b, routes, capacity, [(slot,)]),
        sds(2 * capacity, columns),
        where,
        arrived[slot],
        swapped[slot],
            )
            pieces += spread(picked, 1 + slot % 2)
        hidden = call(
            functools.partial(gate_up_kernel, tp_devices, len(slots)),
            sds(total, units),
            where,
            gain_parts,
            expert_gate,
            expert_up,
            *pieces,
            fetched[1],
            scratch=[pltpu.VMEM((total, model), bf16)],
            limit=16,
        )
        own_side, other_side = call(
            functools.partial(down_kernel, tp_devices, capacity),
            [sds(capacity * len(slots), columns)] * 2,
            where,
            expert_down,
            *spread_direct(hidden),
            scratch=[pltpu.VMEM((total, units * tp_devices), bf16)],
            limit=12,
        )
        mixed = call(
        functools.partial(combine_kernel, len(slots), count_b, capacity, routes),
        [sds(count_b, columns)] * len(slots),
        where,
        *[arrived[slot] for slot in slots],
        own_side,
        over_ep(other_side, 0, 1),
        scratch=[pltpu.VMEM((2 * capacity, columns), bf16)],
        )
        for slot, part in zip(slots, mixed):
            mixes[slot] = over_ep(part, slot) if slot else part

    pair_shape = (2 * count_a, width)
    starts = call(
        functools.partial(near_attention_kernel, count_a, width),
        [jax.ShapeDtypeStruct(pair_shape, f32)] * 6,
        where,
        *mine[:2],
        *theirs[:2],
        limit=14,
        scratch=[
            pltpu.VMEM((2, *pair_shape), bf16),
            pltpu.VMEM((2, *pair_shape), bf16),
            pltpu.VMEM(pair_shape, bf16),
            pltpu.VMEM((2, 2 * count_a, 2 * count_a), f32),
        ],
    )
    head_outs = call(
        functools.partial(attention_kernel, chips, count_a, width),
        [sds(count_a, width)] * chips,
        where,
        second_scale,
        head_gain.reshape(1, width),
        *mine,
        *theirs,
        *starts,
        scalars=2,
        limit=24,
        scratch=[
            pltpu.VMEM((chips, *pair_shape), bf16),
            pltpu.VMEM((chips, *pair_shape), bf16),
            pltpu.VMEM(pair_shape, bf16),
            pltpu.VMEM((chips, 2 * count_a, 2 * count_a), f32),
            *[pltpu.VMEM(pair_shape, f32)] * 3,
        ],
    )
    back = [head_outs[0]] + [over_ep(head_outs[slot], slot) for slot in range(1, chips)]
    pieces = []
    for number, group in enumerate(head_groups):
        value = jnp.concatenate([back[slot] for slot in group], axis=1)
        pieces += spread(value, 1 + number)
    mixer_out = call(
        functools.partial(project_kernel, tp_devices, head_groups, width),
        sds(count_a, out_columns),
        where,
        out_weight,
        *pieces,
        scratch=[pltpu.VMEM((count_a, out_weight.shape[0]), bf16)],
        limit=12,
        last=True,
    )
    expert_mix = functools.reduce(
        jnp.add, [mixes[slot].astype(f32) for slot in range(chips)]
    ).astype(bf16)
    return (mixer_out, expert_mix)


row_groups = [(0, 1), (2, 3)]
head_groups = [(0, 1), (2, 3)]


def fast_fits(mesh):
    return mesh.shape["tp"] == 4 and mesh.shape["ep"] == 8


def solution(mesh):
    placed = (
        P("ep", "tp"),
        P("ep", "tp"),
        P("ep", "tp"),
        P("tp"),
        P(),
        P(None, "tp"),
        P("ep", "tp"),
        P(),
        P("ep", None),
        P("ep", None),
        P("ep", None, "tp"),
        P("ep", None, "tp"),
        P("ep", None, "tp"),
    )
    fast = fast_fits(mesh)

    def body(*args):
        if not fast:
            return per_device(*args)
        return per_device_fast(*args)

    return jax.shard_map(
        body,
        mesh=mesh,
        in_specs=placed,
        out_specs=(P("ep", "tp"), P("ep", "tp")),
        check_vma=False,
    )
```

```python
import functools

import jax
import jax.numpy as jnp
from jax import lax
from jax.experimental import pallas as pl
from jax.experimental.pallas import tpu as pltpu
from jax.sharding import PartitionSpec as P


eps = 1e-06
head_factor = 0.8
neg_big = -1e30
key_block_rows = 1024


def rms_rows(rows_in, gain):
    floats = rows_in.astype(jnp.float32)
    factor = lax.rsqrt(jnp.mean(floats * floats, axis=-1, keepdims=True) + eps)
    return (floats * factor * gain).astype(jnp.bfloat16)


def per_device(
    query_rows,
    key_rows,
    value_rows,
    second_scale,
    head_gain,
    out_weight,
    routed_rows,
    norm_gain,
    route_ids,
    route_weight,
    expert_gate,
    expert_up,
    expert_down,
):
    count_a = query_rows.shape[0]
    per_head = second_scale.shape[0]
    head_dim = query_rows.shape[1] // (2 * per_head)
    value_dim = head_gain.shape[0]
    query_four = query_rows.reshape(count_a, per_head, 2, head_dim)
    query_pos = lax.axis_index("ep") * count_a + jnp.arange(count_a, dtype=jnp.int32)

    def key_block(carry_state, key_part, value_part, block_start):
        key_count = key_part.shape[0]
        key_four = key_part.reshape(key_count, per_head, 2, head_dim)
        value_three = value_part.reshape(key_count, per_head, value_dim)
        scores = jnp.einsum(
            "ihcd,jhcd->ihcj", query_four, key_four, preferred_element_type=jnp.float32
        ) * head_dim ** (-0.5)
        allowed = (
            query_pos[:, None] >= block_start + jnp.arange(key_count, dtype=jnp.int32)[None, :]
        )[:, None, None, :]
        scores = jnp.where(allowed, scores, neg_big)
        old_max, old_sum, old_acc = carry_state
        new_max = jnp.maximum(old_max, jnp.max(scores, axis=-1))
        weights = jnp.where(allowed, jnp.exp(scores - new_max[..., None]), 0.0)
        shrink = jnp.exp(old_max - new_max)
        new_sum = old_sum * shrink + jnp.sum(weights, axis=-1)
        update = jnp.einsum(
            "ihcj,jhe->ihce",
            weights.astype(jnp.bfloat16),
            value_three,
            preferred_element_type=jnp.float32,
        )
        return (new_max, new_sum, old_acc * shrink[..., None] + update)

    start_state = (
        jnp.full((count_a, per_head, 2), neg_big, jnp.float32),
        jnp.zeros((count_a, per_head, 2), jnp.float32),
        jnp.zeros((count_a, per_head, 2, value_dim), jnp.float32),
    )
    key_part = lax.all_gather(key_rows, "ep", axis=0, tiled=True)
    value_part = lax.all_gather(value_rows, "ep", axis=0, tiled=True)
    key_count = key_part.shape[0]

    def step_block(block_num, inner_state):
        offset_rows = block_num * key_block_rows
        key_slice = lax.dynamic_slice_in_dim(key_part, offset_rows, key_block_rows, 0)
        value_slice = lax.dynamic_slice_in_dim(value_part, offset_rows, key_block_rows, 0)
        return key_block(inner_state, key_slice, value_slice, offset_rows)

    _, run_sum, run_acc = lax.fori_loop(0, key_count // key_block_rows, step_block, start_state)
    maps_both = run_acc / run_sum[..., None]
    mixed_maps = maps_both[:, :, 0] - second_scale[None, :, None] * maps_both[:, :, 1]
    mean_sq = jnp.mean(mixed_maps * mixed_maps, axis=-1, keepdims=True)
    head_out = (
        (mixed_maps * lax.rsqrt(mean_sq + eps) * head_gain * head_factor)
        .astype(jnp.bfloat16)
        .reshape(count_a, per_head * value_dim)
    )
    count_b = routed_rows.shape[0]
    route_count = route_ids.shape[1]
    experts_here = expert_gate.shape[0]
    ep_devices = lax.axis_size("ep")
    expert_total = experts_here * ep_devices
    capacity = 2 * count_b * route_count // expert_total
    flat_expert = route_ids.reshape(-1)
    chosen = (flat_expert[:, None] == jnp.arange(expert_total, dtype=jnp.int32)[None, :]).astype(
        jnp.int32
    )
    ranks = jnp.sum((jnp.cumsum(chosen, axis=0) - 1) * chosen, axis=1)
    slot_of = flat_expert * capacity + ranks
    token_of = jnp.arange(count_b * route_count, dtype=jnp.int32) // route_count
    slot_token = jnp.full((expert_total * capacity,), count_b, jnp.int32).at[slot_of].set(token_of)
    padded = jnp.concatenate(
        [routed_rows, jnp.zeros((1, routed_rows.shape[1]), jnp.bfloat16)], axis=0
    )
    outgoing = padded[slot_token].reshape(ep_devices, experts_here, capacity, routed_rows.shape[1])
    column_parts = lax.all_to_all(outgoing, "ep", split_axis=0, concat_axis=0, tiled=True)
    arrived = rms_rows(lax.all_gather(column_parts, "tp", axis=3, tiled=True), norm_gain)
    gate_val = jnp.einsum(
        "sxcd,xdf->sxcf", arrived, expert_gate, preferred_element_type=jnp.float32
    )
    up_val = jnp.einsum("sxcd,xdf->sxcf", arrived, expert_up, preferred_element_type=jnp.float32)
    hidden = (jax.nn.silu(gate_val) * up_val).astype(jnp.bfloat16)
    weight_rows = out_weight
    attn_total = jnp.dot(
        lax.all_gather(
            head_out.reshape(1, 1, count_a, head_out.shape[1]), "tp", axis=3, tiled=True
        )[0, 0],
        weight_rows,
        preferred_element_type=jnp.float32,
    )
    weight_rows = expert_down
    moe_total = jnp.einsum(
        "sxcf,xfd->sxcd",
        lax.all_gather(hidden, "tp", axis=3, tiled=True),
        weight_rows,
        preferred_element_type=jnp.float32,
    )
    mixer_out = attn_total.astype(jnp.bfloat16)
    returned = lax.all_to_all(
        moe_total.astype(jnp.bfloat16), "ep", split_axis=0, concat_axis=0, tiled=True
    )
    flat_back = returned.reshape(expert_total * capacity, returned.shape[3])
    picked = flat_back[slot_of].astype(jnp.float32).reshape(count_b, route_count, returned.shape[3])
    expert_mix = jnp.sum(picked * route_weight[:, :, None], axis=1).astype(jnp.bfloat16)
    return (mixer_out, expert_mix)


bf16 = jnp.bfloat16
f32 = jnp.float32
vmem = pl.BlockSpec(memory_space=pltpu.VMEM)
smem = pl.BlockSpec(memory_space=pltpu.SMEM)


def params(limit):
    return pltpu.CompilerParams(vmem_limit_bytes=limit * 1024 * 1024)


def near_shapes(tree):
    return jax.tree.map(lambda leaf: pltpu.VMEM(leaf.shape, leaf.dtype), tree)


def sds(*shape):
    return jax.ShapeDtypeStruct(shape, bf16)


def pack_kernel(width, where_ref, q_ref, k_ref, v_ref, _, *refs):
    outs, (queries, sems) = refs[:-2], refs[-2:]
    chip = where_ref[0]
    scale = (width // 2) ** (-0.5)
    heads = [pl.ds(pl.multiple_of((chip ^ slot) * width, width), width) for slot in range(len(outs))]
    copies = [pltpu.make_async_copy(q_ref, queries, sems.at[0])]
    for slot, out in enumerate(outs):
        for i, ref in ((1, k_ref), (2, v_ref)):
            at = out.at[:, i * width : (i + 1) * width]
            sem = sems.at[2 * slot + i]
            copies.append(pltpu.make_async_copy(ref.at[:, heads[slot]], at, sem))
    for copy in copies:
        copy.start()
    copies[0].wait()
    for slot, out in enumerate(outs):
        out[:, 0:width] = (queries[:, heads[slot]].astype(f32) * scale).astype(bf16)
    for copy in copies[1:]:
        copy.wait()


def fill_keys(chip, core, base, count, width, own, other, keys, values):
    for slot in range(len(own)):
        at = (chip ^ slot) - base
        for parity, part in ((core, own[slot]), (1 - core, other[slot])):
            rows = pl.ds(pl.multiple_of(parity * count, count), count)
            keys[at, rows] = part[:, width : 2 * width]
            values[at, rows] = part[:, 2 * width : 3 * width]


def softmax_rows(rows, keys, values, queries, scores, state, upto, core, start=None):
    acc, row_max, row_sum = state
    count, width = rows.shape
    half, pair = width // 2, 2 * count
    lane = lax.broadcasted_iota(jnp.int32, (count, width), 1)
    queries[0:count] = jnp.where(lane < half, rows, jnp.zeros_like(rows))
    queries[count:pair] = jnp.where(lane < half, jnp.zeros_like(rows), rows)

    def widest(block):
        best = block[:, 0:width]
        for i in range(width, pair, width):
            best = jnp.maximum(best, block[:, i : i + width])
        return best

    def products(number):
        return lax.dot_general(
            queries[...], keys[number], (((1,), (1,)), ((), ())), preferred_element_type=f32
        )

    def weigh(number):
        top = row_max[...]
        block = [jnp.exp(scores[number, :, i : i + width] - top) for i in range(0, pair, width)]
        total = functools.reduce(jnp.add, block)
        weights = jnp.concatenate([part.astype(bf16) for part in block], axis=1)
        return total, jnp.dot(weights, values[number], preferred_element_type=f32)

    if start is None:
        allowed = lax.broadcasted_iota(jnp.int32, (pair, pair), 1) <= (
            lax.broadcasted_iota(jnp.int32, (pair, pair), 0) % count + core * count
        )
        masked = jnp.where(allowed, products(upto), neg_big)
        scores[upto] = masked
        row_max[...] = widest(masked)
    else:
        row_max[...] = start[1][...]

    @pl.loop(0, upto)
    def _(number):
        block = products(number)
        scores[number] = block
        row_max[...] = jnp.maximum(row_max[...], widest(block))

    row_max[...] = jnp.broadcast_to(
        jnp.max(row_max[...], axis=-1, keepdims=True), row_max.shape
    )
    if start is None:
        row_sum[...], acc[...] = weigh(upto)
    else:
        shrink = jnp.exp(start[1][...] - row_max[...])
        acc[...] = start[0][...] * shrink
        row_sum[...] = start[2][...] * shrink

    @pl.loop(0, upto)
    def _(number):
        total, update = weigh(number)
        row_sum[...] += total
        acc[...] += update


def near_attention_kernel(count, width, where_ref, *refs):
    own, other, outs = refs[0:2], refs[2:4], refs[4:10]
    keys, values, queries, scores = refs[10:]
    chip, core = where_ref[0], where_ref[1]
    base = chip // 2 * 2
    fill_keys(chip, core, base, count, width, own, other, keys, values)
    for slot in range(2):
        state = outs[3 * slot : 3 * slot + 3]
        last = (chip ^ slot) - base
        rows = own[slot][:, 0:width]
        softmax_rows(rows, keys, values, queries, scores, state, last, core)


def attention_kernel(chips, count, width, where_ref, scale_ref, gain_ref, *refs):
    own, other = refs[:chips], refs[chips : 2 * chips]
    starts = refs[2 * chips : 2 * chips + 6]
    outs = refs[2 * chips + 6 : 3 * chips + 6]
    keys, values, queries, scores, acc, row_max, row_sum = refs[3 * chips + 6 :]
    chip, core = where_ref[0], where_ref[1]
    pair = 2 * count
    fill_keys(chip, core, 0, count, width, own, other, keys, values)
    for slot in range(chips):
        start = starts[3 * slot : 3 * slot + 3] if slot < 2 else None
        upto = chip // 2 * 2 if slot < 2 else chip ^ slot
        rows = own[slot][:, 0:width]
        state = (acc, row_max, row_sum)
        softmax_rows(rows, keys, values, queries, scores, state, upto, core, start)
        maps = acc[...] / jnp.sum(row_sum[...], axis=-1, keepdims=True)
        mixed = maps[0:count] - scale_ref[chip] * maps[count:pair]
        mean_sq = jnp.mean(mixed * mixed, axis=-1, keepdims=True)
        outs[slot][...] = (
            mixed * lax.rsqrt(mean_sq + eps) * gain_ref[...] * head_factor
        ).astype(bf16)


def fetch_kernel(value_ref, out):
    out[...] = value_ref[0, 0:8, 0:128]


def fill_heads(parts, slots, width, pieces, heads):
    for part in range(parts):
        for i in range(len(slots)):
            at = (part * len(slots) + i) * width
            heads[:, at : at + width] = pieces[part][:, i * width : (i + 1) * width]


def project_first_kernel(parts, groups, width, where_ref, w_ref, *refs):
    pieces, (out, later, heads, rows) = refs[:parts], refs[parts:]
    chip, tp = where_ref[0], where_ref[2]
    depth = w_ref.shape[0] // parts
    for slots, held in ((groups[0], rows), (groups[1], later)):
        for part in range(parts):
            for i, slot in enumerate(slots):
                source = pl.multiple_of((tp ^ part) * depth + (chip ^ slot) * width, width)
                at = (part * len(slots) + i) * width
                held[at : at + width] = w_ref[pl.ds(source, width)]
    fill_heads(parts, groups[0], width, pieces, heads)
    out[...] = jnp.dot(heads[...], rows[...], preferred_element_type=f32)


def project_kernel(parts, slots, width, first_ref, w_ref, *refs):
    pieces, (out, heads) = refs[:parts], refs[parts:]
    fill_heads(parts, slots, width, pieces, heads)
    product = jnp.dot(heads[...], w_ref[...], preferred_element_type=f32)
    out[...] = (first_ref[...] + product).astype(bf16)


def rows_kernel(count, rows_ref, ids_ref, share_ref, out, ids, share, sems):
    copies = [
        pltpu.make_async_copy(rows_ref, out.at[0:count], sems.at[0]),
        pltpu.make_async_copy(ids_ref, ids, sems.at[1]),
        pltpu.make_async_copy(share_ref, share, sems.at[2]),
    ]
    for copy in copies:
        copy.start()
    out[count:] = jnp.zeros((out.shape[0] - count, out.shape[1]), bf16)
    copies[1].wait()
    copies[2].wait()
    table, rest = [ids[...].astype(f32)], share[...]
    for _ in range(3):
        table.append(rest.astype(bf16).astype(f32))
        rest = rest - table[-1]
    out[count:, 0:count] = jnp.concatenate(table, axis=0).astype(bf16)
    copies[0].wait()


def select_kernel(count, routes, capacity, groups, where_ref, *refs):
    slots = [slot for group in groups for slot in group]
    own, other, outs = refs[: len(slots)], refs[len(slots) : 2 * len(slots)], refs[2 * len(slots) :]
    expert = (2 * where_ref[0] + where_ref[1]).astype(f32)
    before = (
        lax.broadcasted_iota(jnp.int32, (count, count), 0)
        < lax.broadcasted_iota(jnp.int32, (count, count), 1)
    ).astype(f32).astype(bf16)
    row_of = lax.broadcasted_iota(jnp.int32, (capacity, count), 0).astype(f32)
    at = 0
    for out, group in zip(outs, groups):
        for i in range(len(group)):
            for side, part in ((0, own[at]), (1, other[at])):
                ids = part[count : count + 8, 0:count].astype(f32)
                chosen = jnp.zeros((1, count), f32)
                for k in range(routes):
                    chosen = jnp.where(ids[k : k + 1] == expert, 1.0, chosen)
                rank = jnp.dot(
                    jnp.broadcast_to(chosen, (8, count)).astype(bf16),
                    before,
                    preferred_element_type=f32,
                )[0:1]
                rank = jnp.where(chosen > 0, rank, -1.0)
                pick = jnp.where(row_of == rank, 1.0, 0.0).astype(bf16)
                first = (2 * i + side) * capacity
                out[first : first + capacity] = jnp.dot(
                    pick, part[0:count], preferred_element_type=f32
                ).astype(bf16)
            at += 1


def gate_up_kernel(parts, groups, where_ref, gain_ref, gate_ref, up_ref, *refs):
    pieces, (out, rows) = refs[: groups * parts], refs[-2:]
    tp = where_ref[2]
    width = rows.shape[1] // parts
    count = rows.shape[0] // groups
    factors = []
    for group in range(groups):
        square = jnp.zeros((count, 128), f32)
        for part in range(parts):
            floats = pieces[group * parts + part][...].astype(f32)
            for i in range(0, width, 128):
                square = square + floats[:, i : i + 128] * floats[:, i : i + 128]
            at = pl.ds(pl.multiple_of((tp ^ part) * width, width), width)
            rows[group * count : (group + 1) * count, at] = (
                floats * gain_ref[tp ^ part]
            ).astype(bf16)
        mean = jnp.sum(square, axis=-1, keepdims=True) * (1.0 / rows.shape[1])
        factors.append(lax.rsqrt(mean + eps))
    factor = jnp.concatenate(factors, axis=0)
    g = jnp.dot(rows[...], gate_ref[0], preferred_element_type=f32) * factor
    u = jnp.dot(rows[...], up_ref[0], preferred_element_type=f32) * factor
    out[...] = (g / (1.0 + jnp.exp(-g)) * u).astype(bf16)


def down_kernel(parts, capacity, where_ref, w_ref, *refs):
    pieces, (own_out, other_out, rows) = refs[:parts], refs[-3:]
    tp = where_ref[2]
    width = rows.shape[1] // parts
    for part in range(parts):
        rows[:, pl.ds(pl.multiple_of((tp ^ part) * width, width), width)] = pieces[part][...]
    total = jnp.dot(rows[...], w_ref[0], preferred_element_type=f32).astype(bf16)
    for i in range(total.shape[0] // capacity):
        at = i // 2 * capacity
        (own_out, other_out)[i % 2][at : at + capacity] = total[i * capacity : (i + 1) * capacity]


def combine_kernel(chips, count, capacity, routes, where_ref, *refs):
    ids_refs, mine_ref, theirs_ref = refs[:chips], refs[chips], refs[chips + 1]
    outs, rows = refs[chips + 2 : 2 * chips + 2], refs[-1]
    chip, core = where_ref[0], where_ref[1]
    before = (
        lax.broadcasted_iota(jnp.int32, (count, count), 0)
        < lax.broadcasted_iota(jnp.int32, (count, count), 1)
    ).astype(f32).astype(bf16)
    row_of = lax.broadcasted_iota(jnp.int32, (capacity, count), 0).astype(f32)
    for slot, out in enumerate(outs):
        part = ids_refs[slot][count : count + 8, 0:count].astype(f32)
        terms = [[], [], []]
        for side, results in ((0, mine_ref), (1, theirs_ref)):
            rows[side * capacity : (side + 1) * capacity] = results[
                slot * capacity : (slot + 1) * capacity
            ]
            expert = (2 * chip + (core ^ side)).astype(f32)
            chosen = jnp.zeros((1, count), f32)
            share = [jnp.zeros((1, count), f32)] * 3
            for k in range(routes):
                same = part[k : k + 1] == expert
                chosen = jnp.where(same, 1.0, chosen)
                for i in range(3):
                    at = routes * (1 + i) + k
                    share[i] = jnp.where(same, part[at : at + 1], share[i])
            rank = jnp.dot(
                jnp.broadcast_to(chosen, (8, count)).astype(bf16),
                before,
                preferred_element_type=f32,
            )[0:1]
            rank = jnp.where(chosen > 0, rank, -1.0)
            for i in range(3):
                terms[i].append(jnp.where(row_of == rank, share[i], 0.0).astype(bf16))
        total = jnp.zeros(out.shape, f32)
        for i in range(3):
            total = total + lax.dot_general(
                jnp.concatenate(terms[i], axis=0),
                rows[...],
                (((0,), (0,)), ((), ())),
                preferred_element_type=f32,
            )
        out[...] = total.astype(bf16)


def per_device_fast(
    query_rows,
    key_rows,
    value_rows,
    second_scale,
    head_gain,
    out_weight,
    routed_rows,
    norm_gain,
    route_ids,
    route_weight,
    expert_gate,
    expert_up,
    expert_down,
):
    ep_devices, tp_devices = lax.axis_size("ep"), lax.axis_size("tp")
    chips = ep_devices // 2
    count_a, count_b = query_rows.shape[0], routed_rows.shape[0]
    heads_here = second_scale.shape[0]
    width = query_rows.shape[1] // heads_here
    columns = routed_rows.shape[1]
    model = columns * tp_devices
    routes = route_ids.shape[1]
    capacity = 2 * count_b * routes // ep_devices
    units = expert_gate.shape[2]
    out_columns = out_weight.shape[1]
    ep_at = lax.axis_index("ep")
    where = jnp.stack([ep_at // 2, ep_at % 2, lax.axis_index("tp")]).astype(jnp.int32)

    def over_ep(value, slot, cross=0):
        pairs = [(i, (((i // 2) ^ slot) * 2 + (i % 2)) ^ cross) for i in range(ep_devices)]
        return lax.ppermute(value, "ep", pairs)

    def over_tp(value, offset):
        return lax.ppermute(value, "tp", [(i, i ^ offset) for i in range(tp_devices)])

    def spread(value, first):
        second = 3 ^ first
        one = over_tp(value, first)
        two = over_tp(value, second)
        pieces = {0: value, first: one, second: two, 3: over_tp(one, second)}
        return [pieces[offset] for offset in range(tp_devices)]

    def spread_direct(value):
        return [value] + [over_tp(value, offset) for offset in range(1, tp_devices)]

    def call(body, out_shape, *args, scratch=(), scalars=1, limit=8, last=False, far=()):
        far_spec = pl.BlockSpec(memory_space=pltpu.HBM)
        specs = [vmem if i not in far else far_spec for i in range(len(args) - scalars)]
        placed = [
            pltpu.with_memory_space_constraint(value, pltpu.HBM if i in far else pltpu.VMEM)
            for i, value in enumerate(args[scalars:])
        ]
        return pl.pallas_call(
            body,
            out_shape=out_shape if last else near_shapes(out_shape),
            in_specs=[smem] * scalars + specs,
            out_specs=jax.tree.map(lambda _: vmem, out_shape),
            scratch_shapes=list(scratch),
            compiler_params=params(limit),
        )(*args[:scalars], *placed)

    far = [
        pltpu.with_memory_space_constraint(value, pltpu.HBM)
        for value in (routed_rows, route_ids.T, route_weight.T)
    ]
    packed = pl.pallas_call(
        functools.partial(rows_kernel, count_b),
        out_shape=pltpu.VMEM((count_b + 4 * routes, columns), bf16),
        in_specs=[pl.BlockSpec(memory_space=pltpu.HBM)] * 3,
        out_specs=vmem,
        scratch_shapes=[
            pltpu.VMEM((routes, count_b), jnp.int32),
            pltpu.VMEM((routes, count_b), f32),
            pltpu.SemaphoreType.DMA((3,)),
        ],
        compiler_params=params(8),
    )(*far)
    arrived = [packed] + [over_ep(packed, slot) for slot in range(1, chips)]
    swapped = [over_ep(part, 0, 1) for part in arrived]

    fetched = [
        call(fetch_kernel, sds(8, 128), value, scalars=0)
        for value in (expert_gate, expert_up)
    ]

    packs = pl.pallas_call(
        functools.partial(pack_kernel, width),
        out_shape=[pltpu.VMEM((count_a, 3 * width), bf16)] * chips,
        in_specs=[smem] + [pl.BlockSpec(memory_space=pltpu.HBM)] * 3 + [vmem],
        out_specs=[vmem] * chips,
        scratch_shapes=[
            pltpu.VMEM(query_rows.shape, bf16),
            pltpu.SemaphoreType.DMA((2 * chips + 1,)),
        ],
        compiler_params=params(8),
    )(
        where,
        *[
            pltpu.with_memory_space_constraint(value, pltpu.HBM)
            for value in (query_rows, key_rows, value_rows)
        ],
        fetched[0],
    )
    mine = [packs[0]] + [over_ep(packs[slot], slot) for slot in range(1, chips)]
    theirs = [over_ep(part, 0, 1) for part in mine]

    gain_parts = norm_gain.reshape(tp_devices, 1, columns)
    mixes = {}
    for slots in row_groups:
        total = 2 * capacity * len(slots)
        pieces = []
        for slot in slots:
            picked = call(
        functools.partial(select_kernel, count_b, routes, capacity, [(slot,)]),
        sds(2 * capacity, columns),
        where,
        arrived[slot],
        swapped[slot],
            )
            pieces += spread(picked, 1 + slot % 2)
        hidden = call(
            functools.partial(gate_up_kernel, tp_devices, len(slots)),
            sds(total, units),
            where,
            gain_parts,
            expert_gate,
            expert_up,
            *pieces,
            fetched[1],
            scratch=[pltpu.VMEM((total, model), bf16)],
            limit=16,
        )
        own_side, other_side = call(
            functools.partial(down_kernel, tp_devices, capacity),
            [sds(capacity * len(slots), columns)] * 2,
            where,
            expert_down,
            *spread_direct(hidden),
            scratch=[pltpu.VMEM((total, units * tp_devices), bf16)],
            limit=12,
        )
        mixed = call(
        functools.partial(combine_kernel, len(slots), count_b, capacity, routes),
        [sds(count_b, columns)] * len(slots),
        where,
        *[arrived[slot] for slot in slots],
        own_side,
        over_ep(other_side, 0, 1),
        scratch=[pltpu.VMEM((2 * capacity, columns), bf16)],
        )
        for slot, part in zip(slots, mixed):
            mixes[slot] = over_ep(part, slot) if slot else part

    pair_shape = (2 * count_a, width)
    starts = call(
        functools.partial(near_attention_kernel, count_a, width),
        [jax.ShapeDtypeStruct(pair_shape, f32)] * 6,
        where,
        *mine[:2],
        *theirs[:2],
        limit=14,
        scratch=[
            pltpu.VMEM((2, *pair_shape), bf16),
            pltpu.VMEM((2, *pair_shape), bf16),
            pltpu.VMEM(pair_shape, bf16),
            pltpu.VMEM((2, 2 * count_a, 2 * count_a), f32),
        ],
    )
    head_outs = call(
        functools.partial(attention_kernel, chips, count_a, width),
        [sds(count_a, width)] * chips,
        where,
        second_scale,
        head_gain.reshape(1, width),
        *mine,
        *theirs,
        *starts,
        scalars=2,
        limit=24,
        scratch=[
            pltpu.VMEM((chips, *pair_shape), bf16),
            pltpu.VMEM((chips, *pair_shape), bf16),
            pltpu.VMEM(pair_shape, bf16),
            pltpu.VMEM((chips, 2 * count_a, 2 * count_a), f32),
            *[pltpu.VMEM(pair_shape, f32)] * 3,
        ],
    )
    back = [head_outs[0]] + [over_ep(head_outs[slot], slot) for slot in range(1, chips)]
    pieces = []
    for number, group in enumerate(head_groups):
        value = jnp.concatenate([back[slot] for slot in group], axis=1)
        pieces.append(spread(value, 1 + number))
    depth = tp_devices * len(head_groups[0]) * width
    first, later = call(
        functools.partial(project_first_kernel, tp_devices, head_groups, width),
        [
            jax.ShapeDtypeStruct((count_a, out_columns), f32),
            sds(out_weight.shape[0] - depth, out_columns),
        ],
        where,
        out_weight,
        *pieces[0],
        scratch=[pltpu.VMEM((count_a, depth), bf16), pltpu.VMEM((depth, out_columns), bf16)],
        limit=12,
    )
    mixer_out = call(
        functools.partial(project_kernel, tp_devices, head_groups[1], width),
        sds(count_a, out_columns),
        first,
        later,
        *pieces[1],
        scalars=0,
        scratch=[pltpu.VMEM((count_a, out_weight.shape[0] - depth), bf16)],
        limit=12,
        last=True,
    )
    expert_mix = functools.reduce(
        jnp.add, [mixes[slot].astype(f32) for slot in range(chips)]
    ).astype(bf16)
    return (mixer_out, expert_mix)


row_groups = [(0, 1), (2, 3)]
head_groups = [(0, 1), (2, 3)]


def fast_fits(mesh):
    return mesh.shape["tp"] == 4 and mesh.shape["ep"] == 8


def solution(mesh):
    placed = (
        P("ep", "tp"),
        P("ep", "tp"),
        P("ep", "tp"),
        P("tp"),
        P(),
        P(None, "tp"),
        P("ep", "tp"),
        P(),
        P("ep", None),
        P("ep", None),
        P("ep", None, "tp"),
        P("ep", None, "tp"),
        P("ep", None, "tp"),
    )
    fast = fast_fits(mesh)

    def body(*args):
        if not fast:
            return per_device(*args)
        return per_device_fast(*args)

    return jax.shard_map(
        body,
        mesh=mesh,
        in_specs=placed,
        out_specs=(P("ep", "tp"), P("ep", "tp")),
        check_vma=False,
    )
```
